32 devices in a mesh: rep: 2 (over x), fs: 8 (over z, y), tp: 2 (over core).
Axes of the slice: x: 2, y: 2, z: 4, core: 2. Of those that a mesh axis runs over, the one named last changes fastest.
Arguments:
- layer_in: bfloat16 [16384, 2048], P(('rep', 'fs'), 'tp'), may hold values from -60 to 60
- mix_gain: bfloat16 [2048], P('tp'), may hold values from 0.099609375 to 1.8984375
- pool_weight: float32 [4, 512, 512], P('tp', None, 'fs'), may hold values from -0.25 to 0.25
- pool_scale: float32 [4, 512], P('tp'), may hold values from 0.1 to 1.9
- out_weight: float32 [2048, 2048], P('tp', 'fs'), may hold values from -0.125 to 0.125
- out_scale: float32 [2048], P('tp'), may hold values from 0.1 to 1.9
- channel_gain: bfloat16 [2048], P('tp'), may hold values from 0.099609375 to 1.8984375
- up_weight: float32 [2048, 2816], P('fs', 'tp'), may hold values from -0.125 to 0.125
- up_scale: float32 [2816], P('tp'), may hold values from 0.1 to 1.9
- gate_weight: float32 [2048, 2816], P('fs', 'tp'), may hold values from -0.125 to 0.125
- gate_scale: float32 [2816], P('tp'), may hold values from 0.1 to 1.9
- conv_weight: float32 [3, 2816], P(None, 'tp'), may hold values from -3 to 3
- down_weight: float32 [2816, 2048], P('tp', 'fs'), may hold values from -0.109375 to 0.109375
- down_scale: float32 [2048], P('tp'), may hold values from 0.1 to 1.9
Outputs:
- layer_out: bfloat16 [16384, 2048], P(('rep', 'fs'), 'tp')
The draws below stay inside these ranges and needn't reach their ends.
All inputs are finite; a program needn't handle non-finite values.
Results may differ from the reference program's by a relative error of at most 0.0095.
Values may be sent and summed in bfloat16 or wider, within the bound.
A program may use at most 128 MiB of HBM per device.

```python
import jax
import jax.numpy as jnp
from jax import lax

D = 2048
FF = 2816
GROUPS = 4
GROUP_DIM = 512
LENGTH = 256
TOKENS = 16384
N_FS = 8
N_TP = 2


def draw_layer_in(key, part):
    first, second, third = jax.random.split(jax.random.fold_in(key, 11), 3)
    rising = jnp.exp(jnp.log(3.0) * jnp.arange(D, dtype=jnp.float32) / D)
    column = rising * jax.random.uniform(second, (D,), jnp.float32, 0.5, 1.5)
    base = jnp.clip(jax.random.normal(first, (TOKENS, D), jnp.float32), -4.0, 4.0)
    row_scale = jnp.exp(jax.random.uniform(third, (TOKENS, 1), jnp.float32, jnp.log(0.3), jnp.log(3.0)))
    return (base * column[None] * row_scale).astype(jnp.bfloat16)


def block_scale(stream_key, extent, shards, low, top_value):
    def one(dim, parts):
        heights = jax.random.uniform(jax.random.fold_in(jax.random.fold_in(stream_key, 6), dim), (parts,), jnp.float32, low / len(shards), top_value / len(shards))
        return jnp.repeat(jnp.exp(heights), extent[dim] // parts).reshape((-1,) + (1,) * (len(extent) - dim - 1))

    level = one(*shards[0])
    for cut in shards[1:]:
        level = level * one(*cut)
    return level


def bell_draw(own_key, shape, spread, reach, cuts=(), kind=jnp.bfloat16):
    factor_of = block_scale(own_key, shape, cuts, -0.22, 0.18) if cuts else 1.0
    values = jax.random.normal(own_key, shape, jnp.float32) * spread * factor_of
    return jnp.minimum(jnp.maximum(values, -reach), reach).astype(kind)


def setup_inputs(seed: int = 0) -> dict:
    arg_keys = jax.random.split(jax.random.key(seed), 15)
    layer_in = draw_layer_in(jax.random.fold_in(arg_keys[14], 71), 0)
    mix_gain = jnp.clip(1.0 + 0.18 * jax.random.normal(arg_keys[1], (D,), jnp.float32), 0.099609375, 1.8984375).astype(jnp.bfloat16)
    pool_weight = bell_draw(arg_keys[2], (GROUPS, GROUP_DIM, GROUP_DIM), GROUP_DIM ** -0.5, 0.25, ((0, 2), (2, 8)), jnp.float32)
    pool_scale = jnp.clip(1.0 + 0.18 * jax.random.normal(arg_keys[3], (GROUPS, GROUP_DIM), jnp.float32), 0.1, 1.9)
    out_weight = bell_draw(arg_keys[4], (D, D), D ** -0.5, 0.125, ((0, 2), (1, 8)), jnp.float32)
    out_scale = jnp.clip(1.0 + 0.18 * jax.random.normal(arg_keys[5], (D,), jnp.float32), 0.1, 1.9)
    channel_gain = jnp.clip(1.0 + 0.18 * jax.random.normal(arg_keys[6], (D,), jnp.float32), 0.099609375, 1.8984375).astype(jnp.bfloat16)
    up_weight = bell_draw(arg_keys[7], (D, FF), D ** -0.5, 0.125, ((0, 8), (1, 2)), jnp.float32)
    up_scale = jnp.clip(1.0 + 0.18 * jax.random.normal(arg_keys[8], (FF,), jnp.float32), 0.1, 1.9)
    gate_weight = bell_draw(arg_keys[9], (D, FF), D ** -0.5, 0.125, ((0, 8), (1, 2)), jnp.float32)
    gate_scale = jnp.clip(1.0 + 0.18 * jax.random.normal(arg_keys[10], (FF,), jnp.float32), 0.1, 1.9)
    conv_weight = bell_draw(arg_keys[11], (3, FF), 0.577, 3.0, ((1, 2),), jnp.float32)
    down_weight = bell_draw(arg_keys[12], (FF, D), FF ** -0.5, 0.109375, ((0, 2), (1, 8)), jnp.float32)
    down_scale = jnp.clip(1.0 + 0.18 * jax.random.normal(arg_keys[13], (D,), jnp.float32), 0.1, 1.9)
    return dict(layer_in=layer_in, mix_gain=mix_gain, pool_weight=pool_weight, pool_scale=pool_scale, out_weight=out_weight, out_scale=out_scale, channel_gain=channel_gain, up_weight=up_weight, up_scale=up_scale, gate_weight=gate_weight, gate_scale=gate_scale, conv_weight=conv_weight, down_weight=down_weight, down_scale=down_scale)


EPS = 1e-06

def settle(values):
    return lax.optimization_barrier(values.astype(jnp.bfloat16)).astype(jnp.float32)

def band_table(length, window):
    rows = lax.broadcasted_iota(jnp.int32, (length, length), 0)
    cols = lax.broadcasted_iota(jnp.int32, (length, length), 1)
    lower = jnp.maximum(rows - window // 2, 0)
    upper = jnp.minimum(rows - window // 2 + window, length)
    inside = (cols >= lower) & (cols < upper)
    count = (upper[:, :1] - lower[:, :1]).astype(jnp.float32)
    return (inside.astype(jnp.bfloat16), count)

def partial_sums(left, right):
    part = left.shape[1] // N_TP
    total = jnp.zeros((left.shape[0], right.shape[1]), jnp.float32)
    for index in range(N_TP):
        piece = jnp.dot(left[:, index * part:(index + 1) * part], right[index * part:(index + 1) * part], preferred_element_type=jnp.float32)
        total = total + settle(piece)
    return total

def block_layer(block_in, mix_gain, pool_bf, pool_scale, out_bf, out_scale, channel_gain, up_bf, up_scale, gate_bf, gate_scale, conv_weight, down_bf, down_scale):
    rows = block_in.shape[0]
    seqs = rows // LENGTH
    x32 = block_in.astype(jnp.float32)
    normed = settle(x32 * lax.rsqrt(lax.optimization_barrier(jnp.mean(x32 * x32, axis=1, keepdims=True)) + EPS) * mix_gain.astype(jnp.float32))
    grouped_in = normed.reshape(seqs, LENGTH, GROUPS, GROUP_DIM)
    outputs = []
    for group in range(GROUPS):
        band, count = band_table(LENGTH, 2 ** (group + 1))
        piece = grouped_in[:, :, group, :]
        total = jnp.einsum('ij,sjc->sic', band.astype(jnp.float32), piece)
        outputs.append(settle(total / count[None] - piece))
    pooled = jnp.stack(outputs, axis=2)
    grouped = jnp.einsum('slgc,gcd->slgd', pooled, pool_bf.astype(jnp.float32)) * pool_scale[None, None]
    grouped = settle(grouped).astype(jnp.bfloat16).reshape(rows, D)
    mixer_sum = partial_sums(grouped, out_bf)
    middle = (x32 + mixer_sum * out_scale[None]).astype(jnp.bfloat16)
    m32 = middle.astype(jnp.float32)
    chan_normed = (m32 * lax.rsqrt(lax.optimization_barrier(jnp.mean(m32 * m32, axis=1, keepdims=True)) + EPS) * channel_gain.astype(jnp.float32)).astype(jnp.bfloat16)
    lifted = settle(jnp.dot(chan_normed, up_bf, preferred_element_type=jnp.float32) * up_scale[None])
    gated = jnp.dot(chan_normed, gate_bf, preferred_element_type=jnp.float32) * gate_scale[None]
    padded = jnp.pad(lifted.reshape(seqs, LENGTH, FF), ((0, 0), (1, 1), (0, 0)))
    conv = conv_weight[0] * padded[:, :-2] + conv_weight[1] * padded[:, 1:-1] + conv_weight[2] * padded[:, 2:]
    hidden = (jax.nn.gelu(conv).reshape(rows, FF) * gated).astype(jnp.bfloat16)
    chan_sum = partial_sums(hidden, down_bf)
    return (m32 + chan_sum * down_scale[None]).astype(jnp.bfloat16)

def reference(layer_in, mix_gain, pool_weight, pool_scale, out_weight, out_scale, channel_gain, up_weight, up_scale, gate_weight, gate_scale, conv_weight, down_weight, down_scale):
    pool_bf = pool_weight.astype(jnp.bfloat16)
    out_bf = out_weight.astype(jnp.bfloat16)
    up_bf = up_weight.astype(jnp.bfloat16)
    gate_bf = gate_weight.astype(jnp.bfloat16)
    down_bf = down_weight.astype(jnp.bfloat16)
    blocks = layer_in.reshape(N_FS, TOKENS // N_FS, D)

    def one_block(block_in):
        return block_layer(block_in, mix_gain, pool_bf, pool_scale, out_bf, out_scale, channel_gain, up_bf, up_scale, gate_bf, gate_scale, conv_weight, down_bf, down_scale)
    return lax.map(one_block, blocks).reshape(TOKENS, D)
```

```python
import functools

import jax
import jax.numpy as jnp
from jax import lax
from jax.experimental import pallas as pl
from jax.experimental.pallas import tpu as pltpu
from jax.sharding import PartitionSpec as P

LENGTH = 256
EPS = 1e-06
TILE = 16
MESH = pl.DeviceIdType.MESH

ALONG = (0.78, 0.78, 0.78, 0.78, 0.72)
ACROSS = (0.58, 0.58, 0.58, 0.58, 0.60)


class Chunk:
    def __init__(self, index, buffer, shard, offset, rows, along, across):
        units = rows // TILE
        least = (units + 1) // 2
        self.index, self.buffer, self.shard, self.offset, self.rows = index, buffer, shard, offset, rows
        self.along = TILE * min(max(round(units * along), least), units)
        self.across = min(TILE * max(round(units * across), least), self.along)


def dot(left, right):
    return jnp.dot(left, right, preferred_element_type=jnp.float32)


def layer_kernel(n, chunks, *refs):
    x_in, pool_in, out_in, up_in, gate_in, down_in = refs[:6]
    small_in, o_ref, small = refs[6:14], refs[14], refs[15:23]
    poolb, outb, upb, gateb, downb, s_pool, s_out, s_up, s_gate, s_down = refs[23:33]
    xm, keep, sent, recv, cn, lift, ss, ssr = refs[33:41]
    in_sem, zs, zr, ys, yr, xs, xr, ts, tr = refs[41:]
    mix_gain, pool_scale, out_scale, channel_gain, up_scale, gate_scale, conv_weight, down_scale = small
    buffers = (poolb, outb, upb, gateb, downb)

    rows, half = xm.shape
    width = 2 * half
    seqs = rows // LENGTH
    shards = 2 * n
    blocks, _, block = keep.shape
    hidden_width = lift.shape[1]
    group = poolb.shape[1]
    groups = half // group
    pool_rows = pool_in.shape[0]
    lane = pool_rows // groups

    r, f, core = lax.axis_index("rep"), lax.axis_index("fs"), lax.axis_index("tp")
    a, b = f // 2, f % 2

    def order(j):
        near = jnp.minimum(a, n - 1 - a)
        odd = j % 2
        paired = a + (1 - 2 * odd) * ((j + 1) // 2)
        way = jnp.where(a < n - 1 - a, 1, -1)
        return jnp.where(j <= 2 * near, paired, a + way * (j - near))

    def rows_of(chunk, shard, start, count):
        begin = pl.multiple_of(shard * chunk.shard + chunk.offset + start, TILE)
        return buffers[chunk.buffer].at[pl.ds(begin, count)]

    def z_copy(chunk, s, target, slot):
        part = rows_of(chunk, 2 * s + b, r * (chunk.rows - chunk.along), chunk.along)
        return pltpu.make_async_remote_copy(
            src_ref=part, dst_ref=part, send_sem=zs.at[chunk.index, slot], recv_sem=zr.at[chunk.index, s],
            device_id={"fs": 2 * target + b}, device_id_type=MESH,
        )

    def y_copy(chunk, s, side):
        part = rows_of(chunk, 2 * s + side, r * (chunk.rows - chunk.across), chunk.across)
        return pltpu.make_async_remote_copy(
            src_ref=part, dst_ref=part, send_sem=ys.at[chunk.index, s], recv_sem=yr.at[chunk.index, s],
            device_id={"fs": 2 * a + 1 - b}, device_id_type=MESH,
        )

    def x_copy(chunk, s, kind, end):
        had = chunk.across if kind else chunk.along
        part = rows_of(chunk, 2 * s + (1 - b if kind else b), end * had, chunk.rows - had)
        return pltpu.make_async_remote_copy(
            src_ref=part, dst_ref=part, send_sem=xs.at[chunk.index, kind, s], recv_sem=xr.at[chunk.index, kind, s],
            device_id={"rep": 1 - r}, device_id_type=MESH,
        )

    def onward(s):
        target = jnp.where(s < a, a + 1, a - 1)
        return target, (target >= 0) & (target < n)

    def begin(chunk):
        @pl.when(a < n - 1)
        def _():
            z_copy(chunk, a, a + 1, a).start()

        @pl.when(a > 0)
        def _():
            z_copy(chunk, a, a - 1, n).start()

        y_copy(chunk, a, b).start()

    def z_event(chunk, j):
        s = order(j)
        target, valid = onward(s)
        z_copy(chunk, s, a, s).wait_recv()

        @pl.when(valid)
        def _():
            z_copy(chunk, s, target, s).start()

        y_copy(chunk, s, b).start()
        if chunk.rows > chunk.along:
            x_copy(chunk, s, 0, r).start()

    def y_event(chunk, j):
        s = order(j)
        y_copy(chunk, s, 1 - b).wait_recv()
        if chunk.rows > chunk.across:
            x_copy(chunk, s, 1, r).start()

    def x_wait(chunk, j, kind):
        if kind and chunk.rows > chunk.across:
            x_copy(chunk, order(j), 1, 1 - r).wait_recv()
        if not kind and chunk.rows > chunk.along:
            x_copy(chunk, order(j), 0, 1 - r).wait_recv()

    def arrived(which):
        for chunk in which:
            x_wait(chunk, 0, 1)

            def step(j, carry):
                x_wait(chunk, j, 0)
                x_wait(chunk, j, 1)
                return carry

            lax.fori_loop(1, n, step, 0)

    def finish(chunk):
        @pl.when(a < n - 1)
        def _():
            z_copy(chunk, a, a + 1, a).wait_send()

        @pl.when(a > 0)
        def _():
            z_copy(chunk, a, a - 1, n).wait_send()

        def step(j, carry):
            s = order(j)
            target, valid = onward(s)
            y_copy(chunk, s, b).wait_send()
            if chunk.rows > chunk.across:
                x_copy(chunk, s, 1, r).wait_send()

            @pl.when(j > 0)
            def _():
                if chunk.rows > chunk.along:
                    x_copy(chunk, s, 0, r).wait_send()

                @pl.when(valid)
                def _():
                    z_copy(chunk, s, target, s).wait_send()

            return carry

        lax.fori_loop(0, n, step, 0)

    def stage(which, before, piece, count):
        for chunk in which:
            z_event(chunk, 1)
        for chunk in which:
            y_event(chunk, 0)
        before()

        def step(j, carry):
            def one(q, inner):
                piece(q)
                return inner

            lax.fori_loop((j - 1) * count // (n - 1), j * count // (n - 1), one, 0)

            @pl.when(j < n - 1)
            def _():
                for chunk in which:
                    z_event(chunk, j + 1)
                for chunk in which:
                    y_event(chunk, j)

            return carry

        lax.fori_loop(1, n, step, 0)
        for chunk in which:
            y_event(chunk, n - 1)

    def t_copy(kind, index, src, dst):
        return pltpu.make_async_remote_copy(
            src_ref=src, dst_ref=dst, send_sem=ts.at[kind, index], recv_sem=tr.at[kind, index],
            device_id={"tp": 1 - core}, device_id_type=MESH,
        )

    def span(q):
        return pl.ds(pl.multiple_of(q * LENGTH, LENGTH), LENGTH)

    def norm_copy(kind, q):
        return t_copy(2 * kind, q, ss.at[kind, span(q)], ssr.at[kind, span(q)])

    def mixer_copy(q):
        return t_copy(1, q, sent.at[:, span(q)], recv.at[:, span(q)])

    def cn_copy(q, side):
        return t_copy(3, q, cn.at[side, span(q)], cn.at[side, span(q)])

    def down_copy(index):
        return t_copy(4, index, sent.at[index], recv.at[index])

    def line(ref):
        return ref[...].astype(jnp.float32).reshape(1, -1)

    def sum_squares(kind, q):
        values = xm[span(q)].astype(jnp.float32)
        total = jnp.sum(values * values, axis=1, keepdims=True)
        ss[kind, span(q)] = jnp.broadcast_to(total, (LENGTH, ss.shape[2]))

    def inverse(kind, q):
        norm_copy(kind, q).wait_recv()
        total = ss[kind, span(q)][:, :1] + ssr[kind, span(q)][:, :1]
        return lax.rsqrt(total / width + EPS)

    def pool_piece(q):
        values = xm[span(q)].astype(jnp.float32)
        normed = (values * inverse(0, q) * line(mix_gain)).astype(jnp.bfloat16)
        at = lax.broadcasted_iota(jnp.int32, (LENGTH, LENGTH), 0)
        to = lax.broadcasted_iota(jnp.int32, (LENGTH, LENGTH), 1)
        for local in range(groups):
            reach = jnp.left_shift(jnp.int32(1), core * groups + local)
            lower = jnp.maximum(at - reach, 0)
            upper = jnp.minimum(at + reach, LENGTH)
            band = jnp.where((to >= lower) & (to < upper), 1.0, 0.0).astype(jnp.bfloat16)
            count = (upper[:, :1] - lower[:, :1]).astype(jnp.float32)
            part = normed[:, local * group : (local + 1) * group]
            pooled = dot(band, part) / count - part.astype(jnp.float32)
            cn[1 - core, span(q), local * group : (local + 1) * group] = pooled.astype(jnp.bfloat16)

    def mix_piece(q):
        grouped = []
        for local in range(groups):
            pooled = cn[1 - core, span(q), local * group : (local + 1) * group]
            linear = jnp.concatenate(
                [poolb[s * pool_rows + local * lane : s * pool_rows + (local + 1) * lane, :] for s in range(shards)], axis=0
            )
            product = lax.dot_general(pooled, linear, (((1,), (1,)), ((), ())), preferred_element_type=jnp.float32)
            grouped.append((product * pool_scale[local : local + 1, :]).astype(jnp.bfloat16))
        grouped = jnp.concatenate(grouped, axis=1)
        for target, side in ((sent, 1 - core), (keep, core)):

            def one(index, carry):
                start = pl.multiple_of((side * blocks + index) * half, TILE)
                target[index, span(q)] = dot(grouped, outb[pl.ds(start, half), :]).astype(jnp.bfloat16)
                return carry

            lax.fori_loop(0, blocks, one, 0)

    def both(q):
        return jnp.concatenate(
            [keep[i, span(q)].astype(jnp.float32) + recv[i, span(q)].astype(jnp.float32) for i in range(blocks)], axis=1
        )

    def middle_piece(q):
        copy = mixer_copy(q)
        copy.wait_recv()
        copy.wait_send()
        xm[span(q)] = (xm[span(q)].astype(jnp.float32) + both(q) * line(out_scale)).astype(jnp.bfloat16)
        sum_squares(1, q)

    def cn_piece(q):
        values = xm[span(q)].astype(jnp.float32)
        cn[core, span(q)] = (values * inverse(1, q) * line(channel_gain)).astype(jnp.bfloat16)

    def mixer_step(t):
        @pl.when(t >= 2)
        def _():
            cn_piece(t - 2)

        @pl.when((t >= 1) & (t <= seqs))
        def _():
            middle_piece(t - 1)
            norm_copy(1, t - 1).start()

        @pl.when(t < seqs)
        def _():
            mix_piece(t)
            mixer_copy(t).start()

        @pl.when(t >= 2)
        def _():
            cn_copy(t - 2, core).start()

    def wide(q, weight):
        return dot(cn[0, span(q)], weight[:half, :]) + dot(cn[1, span(q)], weight[half:, :])

    def lift_piece(q):
        cn_copy(q, 1 - core).wait_recv()
        lift[span(q)] = (wide(q, upb) * line(up_scale)).astype(jnp.bfloat16)

    def hidden_piece(q):
        gated = wide(q, gateb) * line(gate_scale)
        lifted = lift[span(q)].astype(jnp.float32)
        at = lax.broadcasted_iota(jnp.int32, (LENGTH, 1), 0)
        before = jnp.where(at == 0, 0.0, pltpu.roll(lifted, 1, 0))
        after = jnp.where(at == LENGTH - 1, 0.0, pltpu.roll(lifted, LENGTH - 1, 0))
        conv = (
            conv_weight[0:1, :] * before
            + conv_weight[1:2, :] * lifted
            + conv_weight[2:3, :] * after
        )
        lift[span(q)] = (jax.nn.gelu(conv) * gated).astype(jnp.bfloat16)

    loads = [
        pltpu.make_async_copy(out_in, s_out, in_sem.at[0]),
        pltpu.make_async_copy(pool_in, s_pool, in_sem.at[1]),
        pltpu.make_async_copy(x_in, xm, in_sem.at[2]),
        pltpu.make_async_copy(up_in, s_up, in_sem.at[3]),
        pltpu.make_async_copy(gate_in, s_gate, in_sem.at[4]),
        pltpu.make_async_copy(down_in, s_down, in_sem.at[5]),
    ] + [pltpu.make_async_copy(src, dst, in_sem.at[6 + i]) for i, (src, dst) in enumerate(zip(small_in, small))]
    for load in loads:
        load.start()
    barrier = pltpu.get_barrier_semaphore()
    for peer in ({"rep": 1 - r}, {"fs": 2 * a + 1 - b}, {"tp": 1 - core}):
        pl.semaphore_signal(barrier, inc=1, device_id=peer, device_id_type=MESH)

    @pl.when(a > 0)
    def _():
        pl.semaphore_signal(barrier, inc=1, device_id={"fs": f - 2}, device_id_type=MESH)

    @pl.when(a < n - 1)
    def _():
        pl.semaphore_signal(barrier, inc=1, device_id={"fs": f + 2}, device_id_type=MESH)

    def settle(load, staged, full):
        loads[load].wait()
        count = staged.shape[0]
        full[pl.ds(pl.multiple_of(f * count, TILE), count), :] = staged[...].astype(jnp.bfloat16)

    settle(1, s_pool, poolb)
    settle(0, s_out, outb)
    ends = jnp.where(a > 0, 1, 0) + jnp.where(a < n - 1, 1, 0)
    pl.semaphore_wait(barrier, 3 + ends)

    pool_c, out_c, up_c, gate_c = chunks[:4]
    down_c = chunks[4:]
    begin(pool_c)
    begin(out_c)
    settle(3, s_up, upb)
    for load in loads[2:3] + loads[6:]:
        load.wait()

    def first_sum(q, carry):
        sum_squares(0, q)
        return carry

    lax.fori_loop(0, seqs, first_sum, 0)
    begin(up_c)

    def first_send(q, carry):
        norm_copy(0, q).start()
        return carry

    lax.fori_loop(0, seqs, first_send, 0)
    settle(4, s_gate, gateb)
    settle(5, s_down, downb)

    stage([pool_c, out_c], lambda: None, pool_piece, seqs)
    begin(gate_c)
    stage([up_c], lambda: arrived([pool_c, out_c]), mixer_step, seqs + 2)
    for chunk in down_c:
        begin(chunk)
    stage([gate_c], lambda: arrived([up_c]), lift_piece, seqs)
    stage(down_c, lambda: arrived([gate_c]), hidden_piece, seqs)

    shard_rows = s_down.shape[0]

    def down_step(i, carry):
        j, kind = i // 2, i % 2
        s = order(j)

        @pl.when(kind == 1)
        def _():
            for chunk in down_c:
                x_wait(chunk, j, 1)

        @pl.when((kind == 0) & (j > 0))
        def _():
            for chunk in down_c:
                x_wait(chunk, j, 0)

        shard = 2 * s + (b + kind) % 2
        start = pl.multiple_of(shard * shard_rows, TILE)
        side, index = shard // blocks, shard % blocks
        product = dot(lift[...], downb[pl.ds(start, shard_rows), :]).astype(jnp.bfloat16)

        @pl.when(side == core)
        def _():
            keep[index] = product

        @pl.when(side != core)
        def _():
            sent[index] = product
            down_copy(index).start()

        return carry

    lax.fori_loop(0, shards, down_step, 0)

    def down_wait(index, carry):
        down_copy(index).wait_recv()
        return carry

    lax.fori_loop(0, blocks, down_wait, 0)

    def last(q, carry):
        o_ref[span(q), :] = (xm[span(q)].astype(jnp.float32) + both(q) * line(down_scale)).astype(jnp.bfloat16)
        return carry

    lax.fori_loop(0, seqs, last, 0)

    for chunk in chunks:
        finish(chunk)

    def sends(q, carry):
        norm_copy(0, q).wait_send()
        norm_copy(1, q).wait_send()
        cn_copy(q, core).wait_send()
        return carry

    lax.fori_loop(0, seqs, sends, 0)

    def down_sends(index, carry):
        down_copy(index).wait_send()
        return carry

    lax.fori_loop(0, blocks, down_sends, 0)


def per_device(
    shards,
    layer_in,
    mix_gain,
    pool_weight,
    pool_scale,
    out_weight,
    out_scale,
    channel_gain,
    up_weight,
    up_scale,
    gate_weight,
    gate_scale,
    conv_weight,
    down_weight,
    down_scale,
):
    rows, half = layer_in.shape
    n = shards // 2
    hidden_width = up_weight.shape[1]
    groups, group, lane = pool_weight.shape
    block = out_weight.shape[1]
    blocks = half // block
    seqs = rows // LENGTH
    pool_rows = jnp.transpose(pool_weight, (0, 2, 1)).reshape(groups * lane, group)
    small = (
        mix_gain,
        pool_scale,
        out_scale.reshape(1, -1),
        channel_gain,
        up_scale,
        gate_scale,
        conv_weight,
        down_scale.reshape(1, -1),
    )
    heights = (groups * lane, half, up_weight.shape[0], gate_weight.shape[0])
    chunks = [Chunk(i, i, h, 0, h, ALONG[i], ACROSS[i]) for i, h in enumerate(heights)]
    cut = hidden_width // 2 // TILE * TILE
    for offset, height in ((0, cut), (cut, hidden_width - cut)):
        chunks.append(Chunk(len(chunks), 4, hidden_width, offset, height, ALONG[4], ACROSS[4]))
    count = len(chunks)
    bf16, f32 = jnp.bfloat16, jnp.float32
    dma = pltpu.SemaphoreType.DMA
    return pl.pallas_call(
        functools.partial(layer_kernel, n, chunks),
        out_shape=jax.ShapeDtypeStruct((rows, half), bf16),
        in_specs=[pl.BlockSpec(memory_space=pl.ANY)] * (6 + len(small)),
        out_specs=pl.BlockSpec(memory_space=pltpu.VMEM),
        scratch_shapes=[pltpu.VMEM(v.shape, v.dtype) for v in small]
        + [
            pltpu.VMEM((shards * groups * lane, group), bf16),
            pltpu.VMEM((shards * half, block), bf16),
            pltpu.VMEM((shards * up_weight.shape[0], hidden_width), bf16),
            pltpu.VMEM((shards * gate_weight.shape[0], hidden_width), bf16),
            pltpu.VMEM((shards * hidden_width, block), bf16),
            pltpu.VMEM(pool_rows.shape, f32),
            pltpu.VMEM(out_weight.shape, f32),
            pltpu.VMEM(up_weight.shape, f32),
            pltpu.VMEM(gate_weight.shape, f32),
            pltpu.VMEM(down_weight.shape, f32),
            pltpu.VMEM((rows, half), bf16),
            pltpu.VMEM((blocks, rows, block), bf16),
            pltpu.VMEM((blocks, rows, block), bf16),
            pltpu.VMEM((blocks, rows, block), bf16),
            pltpu.VMEM((2, rows, half), bf16),
            pltpu.VMEM((rows, hidden_width), bf16),
            pltpu.VMEM((2, rows, 128), f32),
            pltpu.VMEM((2, rows, 128), f32),
            dma((6 + len(small),)),
            dma((count, n + 1)),
            dma((count, n)),
            dma((count, n)),
            dma((count, n)),
            dma((count, 2, n)),
            dma((count, 2, n)),
            dma((5, max(seqs, blocks))),
            dma((5, max(seqs, blocks))),
        ],
        compiler_params=pltpu.CompilerParams(
            collective_id=0, has_side_effects=True, vmem_limit_bytes=67_043_328
        ),
        name="layer",
    )(layer_in, pool_rows, out_weight, up_weight, gate_weight, down_weight, *small)


def solution(mesh):
    placed = (
        P(("rep", "fs"), "tp"),
        P("tp"),
        P("tp", None, "fs"),
        P("tp", None),
        P("tp", "fs"),
        P("tp"),
        P("tp"),
        P("fs", "tp"),
        P("tp"),
        P("fs", "tp"),
        P("tp"),
        P(None, "tp"),
        P("tp", "fs"),
        P("tp"),
    )
    body = functools.partial(per_device, mesh.shape["fs"])
    return jax.shard_map(
        body, mesh=mesh, in_specs=placed, out_specs=P(("rep", "fs"), "tp"), check_vma=False
    )
```

```python
import functools

import jax
import jax.numpy as jnp
from jax import lax
from jax.experimental import pallas as pl
from jax.experimental.pallas import tpu as pltpu
from jax.sharding import PartitionSpec as P

LENGTH = 256
EPS = 1e-06
TILE = 16
MESH = pl.DeviceIdType.MESH

PLAN = (
    (0, 0, 1, 0.75, 0.5, 0.5),
    (1, 0, 2, 0.6562, 0.5312, 0.5938),
    (1, 1, 2, 0.7188, 0.5, 0.5),
    (2, 0, 2, 0.625, 0.5, 0.625),
    (2, 1, 2, 0.75, 0.5, 0.625),
    (3, 0, 2, 0.75, 0.5, 0.75),
    (3, 1, 2, 0.75, 0.5, 0.625),
    (4, 0, 4, 0.9091, 0.5455, 0.5),
    (4, 1, 4, 0.9091, 0.5909, 0.6818),
    (4, 2, 4, 0.7727, 0.6364, 0.7273),
    (4, 3, 4, 0.8636, 0.5909, 0.5909),
)
HEAD = 2
SEND, ALONG, ACROSS, ARRIVED = "send", "along", "across", "arrived"

ENDS = (
    ((ACROSS, 0, 0),),
    ((ALONG, 0, 1), (SEND, 2, 0),),
    ((ACROSS, 1, 0),),
    (),
    ((ALONG, 1, 1), (SEND, 3, 0), (ACROSS, 0, 1), (ACROSS, 2, 0), (ALONG, 0, 2), (ALONG, 2, 1), (SEND, 4, 0), (ACROSS, 1, 1), (ACROSS, 3, 0), (ALONG, 1, 2), (ALONG, 3, 1), (SEND, 5, 0), (ACROSS, 2, 1), (ACROSS, 0, 2), (ACROSS, 4, 0), (ALONG, 2, 2), (ALONG, 0, 3), (ACROSS, 3, 1), (ALONG, 4, 1), (SEND, 6, 0), (ACROSS, 1, 2), (ACROSS, 5, 0), (ACROSS, 2, 2), (ALONG, 1, 3), (ALONG, 3, 2), (ALONG, 5, 1), (SEND, 7, 0), (ACROSS, 0, 3), (ACROSS, 4, 1), (ACROSS, 6, 0), (ALONG, 2, 3), (ALONG, 6, 1), (SEND, 8, 0), (ACROSS, 1, 3), (ACROSS, 5, 1), (ACROSS, 3, 2), (ACROSS, 7, 0), (ALONG, 4, 2), (ALONG, 7, 1), (SEND, 9, 0), (ALONG, 3, 3), (ACROSS, 2, 3), (ACROSS, 6, 1), (ACROSS, 8, 0), (ALONG, 5, 2), (ACROSS, 4, 2), (ALONG, 8, 1), (SEND, 10, 0), (ACROSS, 7, 1), (ALONG, 4, 3), (ACROSS, 3, 3), (ACROSS, 9, 0), (ARRIVED, 1, 0),),
    ((ALONG, 9, 1), (ALONG, 6, 2), (ACROSS, 5, 2),),
    ((ALONG, 5, 3),),
    ((ACROSS, 8, 1),),
    ((ACROSS, 10, 0),),
    ((ACROSS, 4, 3),),
    ((ALONG, 7, 2), (ALONG, 6, 3), (ALONG, 10, 1), (ACROSS, 9, 1), (ACROSS, 6, 2), (ACROSS, 5, 3), (ALONG, 8, 2), (ARRIVED, 2, 0),),
    ((ALONG, 7, 3), (ACROSS, 7, 2),),
    ((ALONG, 9, 2),),
    ((ACROSS, 6, 3), (ACROSS, 10, 1),),
    ((ALONG, 8, 3), (ACROSS, 8, 2), (ALONG, 10, 2), (ACROSS, 7, 3), (ALONG, 9, 3), (ARRIVED, 3, 0),),
    ((ACROSS, 9, 2), (ALONG, 10, 3),),
    ((ACROSS, 8, 3),),
    ((ACROSS, 10, 2),),
    ((ACROSS, 9, 3), (ACROSS, 10, 3),),
)
MIDDLES = (
    ((ACROSS, 0, 0),),
    ((ALONG, 0, 1), (SEND, 2, 0), (ALONG, 0, 2),),
    ((ACROSS, 1, 0),),
    (),
    ((ALONG, 1, 1), (SEND, 3, 0), (ALONG, 1, 2), (ACROSS, 0, 1), (ACROSS, 2, 0), (ALONG, 2, 2), (ALONG, 0, 3), (ACROSS, 0, 2), (ALONG, 2, 1), (SEND, 4, 0), (ACROSS, 1, 1), (ALONG, 3, 2), (ACROSS, 3, 0), (ALONG, 3, 1), (SEND, 5, 0), (ALONG, 1, 3), (ACROSS, 1, 2), (ACROSS, 2, 2), (ALONG, 2, 3), (ALONG, 4, 1), (SEND, 6, 0), (ALONG, 4, 2), (ACROSS, 0, 3), (ACROSS, 2, 1), (ACROSS, 4, 0), (ALONG, 5, 1), (SEND, 7, 0), (ALONG, 5, 2), (ALONG, 3, 3), (ACROSS, 3, 1), (ACROSS, 3, 2), (ACROSS, 1, 3), (ACROSS, 5, 0), (ALONG, 6, 1), (SEND, 8, 0), (ALONG, 4, 3), (ALONG, 6, 2), (ALONG, 7, 1), (SEND, 9, 0), (ALONG, 5, 3), (ACROSS, 2, 3), (ACROSS, 4, 1), (ALONG, 7, 2), (ACROSS, 4, 2), (ACROSS, 6, 0), (ALONG, 8, 1), (SEND, 10, 0), (ALONG, 6, 3), (ALONG, 8, 2), (ALONG, 9, 1), (ALONG, 7, 3), (ACROSS, 5, 1), (ACROSS, 5, 2), (ACROSS, 3, 3), (ACROSS, 7, 0), (ALONG, 9, 2), (ALONG, 8, 3), (ALONG, 10, 1), (ALONG, 9, 3), (ACROSS, 6, 1), (ALONG, 10, 2), (ARRIVED, 1, 0),),
    ((ACROSS, 8, 0),),
    ((ACROSS, 6, 2), (ACROSS, 4, 3),),
    ((ALONG, 10, 3),),
    (),
    ((ACROSS, 7, 1),),
    ((ACROSS, 9, 0), (ACROSS, 5, 3), (ACROSS, 7, 2), (ACROSS, 8, 1), (ACROSS, 6, 3), (ACROSS, 10, 0), (ARRIVED, 2, 0),),
    (),
    ((ACROSS, 8, 2),),
    ((ACROSS, 9, 1),),
    ((ACROSS, 7, 3), (ARRIVED, 3, 0),),
    ((ACROSS, 9, 2), (ACROSS, 8, 3),),
    ((ACROSS, 10, 1),),
    (),
    ((ACROSS, 9, 3), (ACROSS, 10, 2), (ACROSS, 10, 3),),
)


class Chunk:
    def __init__(self, index, weight, shard, part, parts, along, across_own, across):
        units = shard // TILE
        first, last = units * part // parts, units * (part + 1) // parts
        count = last - first
        least = (count + 1) // 2
        self.index, self.weight, self.shard = index, weight, shard
        self.offset, self.rows = first * TILE, count * TILE

        def share(fraction, most):
            return TILE * min(max(round(count * fraction), least), most)

        self.along = share(along, count)
        self.across_own = share(across_own, count)
        self.across = share(across, self.along // TILE)


def plain(chunks, n, seqs):
    counts = {0: seqs, 1: seqs + 2, 2: seqs, 3: seqs}
    segments = [[(SEND, chunk.index, 0) for chunk in chunks[HEAD:]]] + [[] for _ in range(seqs)]
    for weight in range(5):
        for chunk in chunks:
            if chunk.weight == weight:
                for j in range(1, n):
                    segments[-1] += [(ALONG, chunk.index, j), (ACROSS, chunk.index, j - 1)]
                segments[-1].append((ACROSS, chunk.index, n - 1))
        if 1 <= weight <= 3:
            segments[-1].append((ARRIVED, weight, 0))
            segments += [[] for _ in range(counts[weight])]
    return segments


def dot(left, right):
    return jnp.dot(left, right, preferred_element_type=jnp.float32)


def layer_kernel(n, chunks, segments, *refs):
    x_in, pool_in, out_in, up_in, gate_in, down_in = refs[:6]
    small_in, o_ref, small = refs[6:14], refs[14], refs[15:23]
    poolb, outb, upb, gateb, downb, s_pool, s_out, s_up, s_gate, s_down = refs[23:33]
    xm, keep, sent, recv, cn, lift, ss, ssr = refs[33:41]
    in_sem, out_sem, zs, zr, ys, yr, xs, xr, ts, tr = refs[41:]
    mix_gain, pool_scale, out_scale, channel_gain, up_scale, gate_scale, conv_weight, down_scale = small
    buffers = (poolb, outb, upb, gateb, downb)

    rows, half = xm.shape
    width = 2 * half
    seqs = rows // LENGTH
    shards = 2 * n
    blocks, _, block = keep.shape
    hidden_width = lift.shape[1]
    group = poolb.shape[1]
    groups = half // group
    pool_rows = pool_in.shape[0]
    lane = pool_rows // groups

    r, f, core = lax.axis_index("rep"), lax.axis_index("fs"), lax.axis_index("tp")
    a, b = f // 2, f % 2

    def order(j):
        near = jnp.minimum(a, n - 1 - a)
        odd = j % 2
        paired = a + (1 - 2 * odd) * ((j + 1) // 2)
        way = jnp.where(a < n - 1 - a, 1, -1)
        return jnp.where(j <= 2 * near, paired, a + way * (j - near))

    def rows_of(chunk, shard, start, count):
        begin = pl.multiple_of(shard * chunk.shard + chunk.offset + start, TILE)
        return buffers[chunk.weight].at[pl.ds(begin, count)]

    def z_copy(chunk, s, target, slot):
        part = rows_of(chunk, 2 * s + b, r * (chunk.rows - chunk.along), chunk.along)
        return pltpu.make_async_remote_copy(
            src_ref=part, dst_ref=part, send_sem=zs.at[chunk.index, slot], recv_sem=zr.at[chunk.index, s],
            device_id={"fs": 2 * target + b}, device_id_type=MESH,
        )

    def y_copy(chunk, s, side, own):
        had = chunk.across_own if own else chunk.across
        part = rows_of(chunk, 2 * s + side, r * (chunk.rows - had), had)
        return pltpu.make_async_remote_copy(
            src_ref=part, dst_ref=part, send_sem=ys.at[chunk.index, s], recv_sem=yr.at[chunk.index, s],
            device_id={"fs": 2 * a + 1 - b}, device_id_type=MESH,
        )

    def x_copy(chunk, s, kind, end, own=False):
        had = chunk.along if kind == 0 else chunk.across_own if own else chunk.across
        part = rows_of(chunk, 2 * s + (1 - b if kind else b), end * had, chunk.rows - had)
        return pltpu.make_async_remote_copy(
            src_ref=part, dst_ref=part, send_sem=xs.at[chunk.index, kind, s], recv_sem=xr.at[chunk.index, kind, s],
            device_id={"rep": 1 - r}, device_id_type=MESH,
        )

    def onward(s):
        target = jnp.where(s < a, a + 1, a - 1)
        return target, (target >= 0) & (target < n)

    def begin(chunk):
        @pl.when(a < n - 1)
        def _():
            z_copy(chunk, a, a + 1, a).start()

        @pl.when(a > 0)
        def _():
            z_copy(chunk, a, a - 1, n).start()

        y_copy(chunk, a, b, True).start()

    def z_event(chunk, j):
        s = order(j)
        target, valid = onward(s)
        z_copy(chunk, s, a, s).wait_recv()

        @pl.when(valid)
        def _():
            z_copy(chunk, s, target, s).start()

        y_copy(chunk, s, b, False).start()
        if chunk.rows > chunk.along:
            x_copy(chunk, s, 0, r).start()

    def y_event(chunk, j):
        s = order(j)
        own = j == 0
        y_copy(chunk, s, 1 - b, own).wait_recv()
        if chunk.rows > (chunk.across_own if own else chunk.across):
            x_copy(chunk, s, 1, r, own).start()

    def x_wait(chunk, j, kind, own=False):
        had = chunk.along if kind == 0 else chunk.across_own if own else chunk.across
        if chunk.rows > had:
            x_copy(chunk, order(j), kind, 1 - r, own).wait_recv()

    def arrived(weights):
        for chunk in chunks:
            if chunk.weight in weights:
                x_wait(chunk, 0, 1, True)

                def step(j, carry):
                    x_wait(chunk, j, 0)
                    x_wait(chunk, j, 1)
                    return carry

                lax.fori_loop(1, n, step, 0)

    def finish(chunk):
        @pl.when(a < n - 1)
        def _():
            z_copy(chunk, a, a + 1, a).wait_send()

        @pl.when(a > 0)
        def _():
            z_copy(chunk, a, a - 1, n).wait_send()

        y_copy(chunk, a, b, True).wait_send()
        if chunk.rows > chunk.across_own:
            x_copy(chunk, a, 1, r, True).wait_send()

        def step(j, carry):
            s = order(j)
            target, valid = onward(s)
            y_copy(chunk, s, b, False).wait_send()
            if chunk.rows > chunk.across:
                x_copy(chunk, s, 1, r).wait_send()
            if chunk.rows > chunk.along:
                x_copy(chunk, s, 0, r).wait_send()

            @pl.when(valid)
            def _():
                z_copy(chunk, s, target, s).wait_send()

            return carry

        lax.fori_loop(1, n, step, 0)

    def events(segment):
        for name, index, j in segment:
            if name == SEND:
                begin(chunks[index])
            elif name == ALONG:
                z_event(chunks[index], j)
            elif name == ACROSS:
                y_event(chunks[index], j)
            else:
                arrived((0, 1) if index == 1 else (index,))

    inner = (a > 0) & (a < n - 1)

    def between(ends, middles):
        if ends == middles:
            events(ends)
            return

        @pl.when(jnp.logical_not(inner))
        def _():
            events(ends)

        @pl.when(inner)
        def _():
            events(middles)

    def stage(first, count, piece):
        def step(q, carry):
            piece(q)
            for i in range(count):
                if segments[0][first + i] or segments[1][first + i]:

                    @pl.when(q == i)
                    def _(i=i):
                        between(segments[0][first + i], segments[1][first + i])

            return carry

        lax.fori_loop(0, count, step, 0)

    def t_copy(kind, index, src, dst):
        return pltpu.make_async_remote_copy(
            src_ref=src, dst_ref=dst, send_sem=ts.at[kind, index], recv_sem=tr.at[kind, index],
            device_id={"tp": 1 - core}, device_id_type=MESH,
        )

    def span(q):
        return pl.ds(pl.multiple_of(q * LENGTH, LENGTH), LENGTH)

    def norm_copy(kind, q):
        return t_copy(2 * kind, q, ss.at[kind, span(q)], ssr.at[kind, span(q)])

    def mixer_copy(q):
        return t_copy(1, q, sent.at[:, span(q)], recv.at[:, span(q)])

    def cn_copy(q, side):
        return t_copy(3, q, cn.at[side, span(q)], cn.at[side, span(q)])

    def down_copy(index):
        return t_copy(4, index, sent.at[index], recv.at[index])

    def line(ref):
        return ref[...].astype(jnp.float32).reshape(1, -1)

    def sum_squares(kind, q):
        values = xm[span(q)].astype(jnp.float32)
        total = jnp.sum(values * values, axis=1, keepdims=True)
        ss[kind, span(q)] = jnp.broadcast_to(total, (LENGTH, ss.shape[2]))

    def inverse(kind, q):
        norm_copy(kind, q).wait_recv()
        total = ss[kind, span(q)][:, :1] + ssr[kind, span(q)][:, :1]
        return lax.rsqrt(total / width + EPS)

    def pool_piece(q):
        values = xm[span(q)].astype(jnp.float32)
        normed = (values * inverse(0, q) * line(mix_gain)).astype(jnp.bfloat16)
        at = lax.broadcasted_iota(jnp.int32, (LENGTH, LENGTH), 0)
        to = lax.broadcasted_iota(jnp.int32, (LENGTH, LENGTH), 1)
        for local in range(groups):
            reach = jnp.left_shift(jnp.int32(1), core * groups + local)
            lower = jnp.maximum(at - reach, 0)
            upper = jnp.minimum(at + reach, LENGTH)
            band = jnp.where((to >= lower) & (to < upper), 1.0, 0.0).astype(jnp.bfloat16)
            count = (upper[:, :1] - lower[:, :1]).astype(jnp.float32)
            part = normed[:, local * group : (local + 1) * group]
            pooled = dot(band, part) / count - part.astype(jnp.float32)
            cn[1 - core, span(q), local * group : (local + 1) * group] = pooled.astype(jnp.bfloat16)

    def mix_piece(q):
        grouped = []
        for local in range(groups):
            pooled = cn[1 - core, span(q), local * group : (local + 1) * group]
            linear = jnp.concatenate(
                [poolb[s * pool_rows + local * lane : s * pool_rows + (local + 1) * lane, :] for s in range(shards)], axis=0
            )
            product = lax.dot_general(pooled, linear, (((1,), (1,)), ((), ())), preferred_element_type=jnp.float32)
            grouped.append((product * pool_scale[local : local + 1, :]).astype(jnp.bfloat16))
        grouped = jnp.concatenate(grouped, axis=1)
        for target, side in ((sent, 1 - core), (keep, core)):

            def one(index, carry):
                start = pl.multiple_of((side * blocks + index) * half, TILE)
                target[index, span(q)] = dot(grouped, outb[pl.ds(start, half), :]).astype(jnp.bfloat16)
                return carry

            lax.fori_loop(0, blocks, one, 0)

    def both(q):
        return jnp.concatenate(
            [keep[i, span(q)].astype(jnp.float32) + recv[i, span(q)].astype(jnp.float32) for i in range(blocks)], axis=1
        )

    def middle_piece(q):
        copy = mixer_copy(q)
        copy.wait_recv()
        copy.wait_send()
        xm[span(q)] = (xm[span(q)].astype(jnp.float32) + both(q) * line(out_scale)).astype(jnp.bfloat16)
        sum_squares(1, q)

    def cn_piece(q):
        values = xm[span(q)].astype(jnp.float32)
        cn[core, span(q)] = (values * inverse(1, q) * line(channel_gain)).astype(jnp.bfloat16)

    def mixer_step(t):
        @pl.when(t >= 2)
        def _():
            cn_piece(t - 2)

        @pl.when((t >= 1) & (t <= seqs))
        def _():
            middle_piece(t - 1)
            norm_copy(1, t - 1).start()

        @pl.when(t < seqs)
        def _():
            mix_piece(t)
            mixer_copy(t).start()

        @pl.when(t >= 2)
        def _():
            cn_copy(t - 2, core).start()

    def wide(q, weight):
        return dot(cn[0, span(q)], weight[:half, :]) + dot(cn[1, span(q)], weight[half:, :])

    def lift_piece(q):
        cn_copy(q, 1 - core).wait_recv()
        lift[span(q)] = (wide(q, upb) * line(up_scale)).astype(jnp.bfloat16)

    def hidden_piece(q):
        gated = wide(q, gateb) * line(gate_scale)
        lifted = lift[span(q)].astype(jnp.float32)
        at = lax.broadcasted_iota(jnp.int32, (LENGTH, 1), 0)
        before = jnp.where(at == 0, 0.0, pltpu.roll(lifted, 1, 0))
        after = jnp.where(at == LENGTH - 1, 0.0, pltpu.roll(lifted, LENGTH - 1, 0))
        conv = (
            conv_weight[0:1, :] * before
            + conv_weight[1:2, :] * lifted
            + conv_weight[2:3, :] * after
        )
        lift[span(q)] = (jax.nn.gelu(conv) * gated).astype(jnp.bfloat16)

    loads = [
        pltpu.make_async_copy(out_in, s_out, in_sem.at[0]),
        pltpu.make_async_copy(pool_in, s_pool, in_sem.at[1]),
        pltpu.make_async_copy(x_in, xm, in_sem.at[2]),
        pltpu.make_async_copy(up_in, s_up, in_sem.at[3]),
        pltpu.make_async_copy(gate_in, s_gate, in_sem.at[4]),
        pltpu.make_async_copy(down_in, s_down, in_sem.at[5]),
    ] + [pltpu.make_async_copy(src, dst, in_sem.at[6 + i]) for i, (src, dst) in enumerate(zip(small_in, small))]
    for load in loads:
        load.start()
    barrier = pltpu.get_barrier_semaphore()
    for peer in ({"rep": 1 - r}, {"fs": 2 * a + 1 - b}, {"tp": 1 - core}):
        pl.semaphore_signal(barrier, inc=1, device_id=peer, device_id_type=MESH)

    @pl.when(a > 0)
    def _():
        pl.semaphore_signal(barrier, inc=1, device_id={"fs": f - 2}, device_id_type=MESH)

    @pl.when(a < n - 1)
    def _():
        pl.semaphore_signal(barrier, inc=1, device_id={"fs": f + 2}, device_id_type=MESH)

    def settle(load, staged, full):
        loads[load].wait()
        count = staged.shape[0]
        full[pl.ds(pl.multiple_of(f * count, TILE), count), :] = staged[...].astype(jnp.bfloat16)

    settle(1, s_pool, poolb)
    settle(0, s_out, outb)
    ends = jnp.where(a > 0, 1, 0) + jnp.where(a < n - 1, 1, 0)
    pl.semaphore_wait(barrier, 3 + ends)

    for chunk in chunks[:HEAD]:
        begin(chunk)
    settle(3, s_up, upb)
    for load in loads[2:3] + loads[6:]:
        load.wait()

    def first_sum(q, carry):
        sum_squares(0, q)
        return carry

    lax.fori_loop(0, seqs, first_sum, 0)

    def first_send(q, carry):
        norm_copy(0, q).start()
        return carry

    lax.fori_loop(0, seqs, first_send, 0)
    settle(4, s_gate, gateb)
    settle(5, s_down, downb)
    between(segments[0][0], segments[1][0])

    stage(1, seqs, pool_piece)
    stage(1 + seqs, seqs + 2, mixer_step)
    stage(3 + 2 * seqs, seqs, lift_piece)
    stage(3 + 3 * seqs, seqs, hidden_piece)
    down_c = [chunk for chunk in chunks if chunk.weight == 4]
    for chunk in chunks:
        if chunk.weight < 3:
            finish(chunk)

    shard_rows = s_down.shape[0]

    def down_step(i, carry):
        j, kind = i // 2, i % 2
        s = order(j)

        @pl.when((kind == 1) & (j == 0))
        def _():
            for chunk in down_c:
                x_wait(chunk, 0, 1, True)

        @pl.when((kind == 1) & (j > 0))
        def _():
            for chunk in down_c:
                x_wait(chunk, j, 1)

        @pl.when((kind == 0) & (j > 0))
        def _():
            for chunk in down_c:
                x_wait(chunk, j, 0)

        shard = 2 * s + (b + kind) % 2
        start = pl.multiple_of(shard * shard_rows, TILE)
        side, index = shard // blocks, shard % blocks
        product = dot(lift[...], downb[pl.ds(start, shard_rows), :]).astype(jnp.bfloat16)

        @pl.when(side == core)
        def _():
            keep[index] = product

        @pl.when(side != core)
        def _():
            sent[index] = product
            down_copy(index).start()

        return carry

    lax.fori_loop(0, shards, down_step, 0)

    def down_wait(index, carry):
        down_copy(index).wait_recv()
        return carry

    lax.fori_loop(0, blocks, down_wait, 0)

    def result(q):
        return pltpu.make_async_copy(xm.at[span(q)], o_ref.at[span(q)], out_sem.at[q])

    def last(q, carry):
        xm[span(q)] = (xm[span(q)].astype(jnp.float32) + both(q) * line(down_scale)).astype(jnp.bfloat16)
        result(q).start()
        return carry

    lax.fori_loop(0, seqs, last, 0)

    for chunk in chunks:
        if chunk.weight >= 3:
            finish(chunk)

    def sends(q, carry):
        norm_copy(0, q).wait_send()
        norm_copy(1, q).wait_send()
        cn_copy(q, core).wait_send()
        result(q).wait()
        return carry

    lax.fori_loop(0, seqs, sends, 0)

    def down_sends(index, carry):
        down_copy(index).wait_send()
        return carry

    lax.fori_loop(0, blocks, down_sends, 0)


def per_device(
    shards,
    layer_in,
    mix_gain,
    pool_weight,
    pool_scale,
    out_weight,
    out_scale,
    channel_gain,
    up_weight,
    up_scale,
    gate_weight,
    gate_scale,
    conv_weight,
    down_weight,
    down_scale,
):
    rows, half = layer_in.shape
    n = shards // 2
    hidden_width = up_weight.shape[1]
    groups, group, lane = pool_weight.shape
    block = out_weight.shape[1]
    blocks = half // block
    seqs = rows // LENGTH
    pool_rows = jnp.transpose(pool_weight, (0, 2, 1)).reshape(groups * lane, group)
    small = (
        mix_gain,
        pool_scale,
        out_scale.reshape(1, -1),
        channel_gain,
        up_scale,
        gate_scale,
        conv_weight,
        down_scale.reshape(1, -1),
    )
    heights = (groups * lane, half, up_weight.shape[0], gate_weight.shape[0], hidden_width)
    chunks = [Chunk(i, entry[0], heights[entry[0]], *entry[1:]) for i, entry in enumerate(PLAN)]
    segments = (ENDS, MIDDLES) if n == 4 and seqs == 4 else (plain(chunks, n, seqs),) * 2
    count = len(chunks)
    bf16, f32 = jnp.bfloat16, jnp.float32
    dma = pltpu.SemaphoreType.DMA
    return pl.pallas_call(
        functools.partial(layer_kernel, n, chunks, segments),
        out_shape=jax.ShapeDtypeStruct((rows, half), bf16),
        in_specs=[pl.BlockSpec(memory_space=pl.ANY)] * (6 + len(small)),
        out_specs=pl.BlockSpec(memory_space=pl.ANY),
        scratch_shapes=[pltpu.VMEM(v.shape, v.dtype) for v in small]
        + [
            pltpu.VMEM((shards * groups * lane, group), bf16),
            pltpu.VMEM((shards * half, block), bf16),
            pltpu.VMEM((shards * up_weight.shape[0], hidden_width), bf16),
            pltpu.VMEM((shards * gate_weight.shape[0], hidden_width), bf16),
            pltpu.VMEM((shards * hidden_width, block), bf16),
            pltpu.VMEM(pool_rows.shape, f32),
            pltpu.VMEM(out_weight.shape, f32),
            pltpu.VMEM(up_weight.shape, f32),
            pltpu.VMEM(gate_weight.shape, f32),
            pltpu.VMEM(down_weight.shape, f32),
            pltpu.VMEM((rows, half), bf16),
            pltpu.VMEM((blocks, rows, block), bf16),
            pltpu.VMEM((blocks, rows, block), bf16),
            pltpu.VMEM((blocks, rows, block), bf16),
            pltpu.VMEM((2, rows, half), bf16),
            pltpu.VMEM((rows, hidden_width), bf16),
            pltpu.VMEM((2, rows, 128), f32),
            pltpu.VMEM((2, rows, 128), f32),
            dma((6 + len(small),)),
            dma((seqs,)),
            dma((count, n + 1)),
            dma((count, n)),
            dma((count, n)),
            dma((count, n)),
            dma((count, 2, n)),
            dma((count, 2, n)),
            dma((5, max(seqs, blocks))),
            dma((5, max(seqs, blocks))),
        ],
        compiler_params=pltpu.CompilerParams(
            collective_id=0, has_side_effects=True, vmem_limit_bytes=67_043_328
        ),
        name="layer",
    )(layer_in, pool_rows, out_weight, up_weight, gate_weight, down_weight, *small)


def solution(mesh):
    placed = (
        P(("rep", "fs"), "tp"),
        P("tp"),
        P("tp", None, "fs"),
        P("tp", None),
        P("tp", "fs"),
        P("tp"),
        P("tp"),
        P("fs", "tp"),
        P("tp"),
        P("fs", "tp"),
        P("tp"),
        P(None, "tp"),
        P("tp", "fs"),
        P("tp"),
    )
    body = functools.partial(per_device, mesh.shape["fs"])
    return jax.shard_map(
        body, mesh=mesh, in_specs=placed, out_specs=P(("rep", "fs"), "tp"), check_vma=False
    )
```

```python
import functools

import jax
import jax.numpy as jnp
from jax import lax
from jax.experimental import pallas as pl
from jax.experimental.pallas import tpu as pltpu
from jax.sharding import PartitionSpec as P

LENGTH = 256
EPS = 1e-06
TILE = 16
MESH = pl.DeviceIdType.MESH

PLAN = (
    (0, 0, 1, 4, 5, 4),
    (1, 0, 2, 16, 17, 16),
    (1, 1, 2, 17, 16, 16),
    (2, 0, 2, 4, 4, 4),
    (2, 1, 2, 6, 4, 4),
    (3, 0, 2, 8, 8, 5),
    (3, 1, 2, 7, 4, 6),
    (4, 0, 4, 20, 11, 17),
    (4, 1, 4, 19, 11, 14),
    (4, 2, 4, 20, 19, 11),
    (4, 3, 4, 22, 17, 12),
)
UNITS = (8, 32, 32, 8, 8, 8, 8, 22, 22, 22, 22)
HEAD = 2
SEND_ALONG, SEND_ACROSS, ALONG, ACROSS, ARRIVED = range(5)

ENDS = (
    ((SEND_ACROSS, 4, 0), (SEND_ALONG, 2, 0), (SEND_ALONG, 3, 0), (ALONG, 0, 1), (SEND_ALONG, 9, 0), (ALONG, 1, 1),
     (ALONG, 0, 2), (ACROSS, 1, 0),),
    ((ALONG, 2, 1), (SEND_ALONG, 6, 0), (ALONG, 1, 2), (SEND_ACROSS, 3, 0), (SEND_ACROSS, 2, 0), (ACROSS, 4, 0),
     (ACROSS, 1, 1), (SEND_ACROSS, 9, 0), (ACROSS, 1, 2), (ALONG, 1, 3), (SEND_ALONG, 4, 0), (ALONG, 4, 1),
     (SEND_ALONG, 10, 0), (ALONG, 2, 3), (SEND_ACROSS, 8, 0), (ACROSS, 2, 1), (ACROSS, 1, 3), (ALONG, 2, 2),
     (SEND_ACROSS, 6, 0), (ACROSS, 0, 1),),
    ((ACROSS, 2, 0), (ACROSS, 0, 0), (ALONG, 7, 1), (ACROSS, 3, 0), (ACROSS, 2, 3), (ALONG, 0, 3), (ALONG, 3, 3),
     (SEND_ACROSS, 10, 0),),
    ((SEND_ACROSS, 5, 0), (ALONG, 3, 1), (ALONG, 6, 1), (ACROSS, 2, 2), (SEND_ALONG, 8, 0), (ACROSS, 0, 2),
     (ACROSS, 10, 0), (ACROSS, 0, 3), (ACROSS, 5, 0), (ACROSS, 6, 0), (ACROSS, 8, 0),),
    ((SEND_ALONG, 5, 0), (ALONG, 9, 3), (SEND_ACROSS, 7, 0), (ALONG, 5, 1), (ACROSS, 4, 1), (ACROSS, 6, 1),
     (ALONG, 4, 2), (ARRIVED, 1, 0), (SEND_ALONG, 7, 0),),
    ((ACROSS, 3, 3), (ALONG, 4, 3), (ALONG, 3, 2),),
    ((ACROSS, 5, 1), (ALONG, 6, 3), (ACROSS, 4, 3), (ACROSS, 7, 1),),
    ((ACROSS, 3, 1), (ALONG, 6, 2), (ALONG, 9, 2), (ACROSS, 3, 2), (ALONG, 5, 2),),
    ((ACROSS, 4, 2), (ACROSS, 6, 2), (ACROSS, 9, 3), (ACROSS, 6, 3), (ALONG, 5, 3), (ALONG, 8, 1),),
    ((ACROSS, 9, 0),),
    ((ARRIVED, 2, 0), (ACROSS, 5, 3), (ACROSS, 5, 2), (ALONG, 9, 1), (ALONG, 8, 2), (ALONG, 10, 1),),
    (),
    ((ALONG, 7, 3), (ALONG, 7, 2), (ACROSS, 7, 0),),
    (),
    ((ACROSS, 8, 2), (ACROSS, 9, 1), (ACROSS, 7, 3), (ALONG, 10, 2), (ACROSS, 10, 1), (ARRIVED, 3, 0),),
    ((ALONG, 10, 3), (ACROSS, 7, 2), (ACROSS, 9, 2), (ACROSS, 8, 1),),
    ((ALONG, 8, 3),),
    ((ACROSS, 10, 2), (ACROSS, 10, 3),),
    ((ACROSS, 8, 3),),
)
MIDDLES = (
    ((ALONG, 0, 2), (SEND_ALONG, 2, 0), (SEND_ACROSS, 10, 0), (ALONG, 1, 1), (ALONG, 1, 2), (ACROSS, 10, 0),
     (ALONG, 2, 1), (SEND_ALONG, 4, 0), (ACROSS, 0, 0), (SEND_ACROSS, 3, 0), (SEND_ALONG, 7, 0), (ALONG, 1, 3),
     (ALONG, 2, 3), (ALONG, 0, 1), (ACROSS, 1, 1), (SEND_ACROSS, 4, 0), (SEND_ALONG, 6, 0), (ALONG, 2, 2),
     (ACROSS, 3, 0), (ACROSS, 0, 2), (ALONG, 3, 1), (ALONG, 0, 3), (SEND_ALONG, 5, 0), (ALONG, 9, 1), (ALONG, 3, 3),
     (SEND_ACROSS, 2, 0), (SEND_ALONG, 3, 0), (ALONG, 4, 1), (ACROSS, 2, 3), (ACROSS, 4, 0), (ALONG, 9, 3),
     (ACROSS, 3, 1), (ALONG, 6, 1), (SEND_ACROSS, 6, 0), (ACROSS, 0, 3), (ALONG, 10, 1),),
    ((ACROSS, 1, 2), (ALONG, 4, 2), (ACROSS, 2, 2), (ACROSS, 2, 0), (ACROSS, 1, 3), (SEND_ACROSS, 5, 0),
     (ALONG, 6, 2), (ALONG, 4, 3), (ACROSS, 0, 1),),
    ((ALONG, 3, 2), (SEND_ALONG, 9, 0), (ACROSS, 1, 0), (ALONG, 9, 2), (ALONG, 6, 3), (ACROSS, 2, 1), (ACROSS, 6, 0),),
    ((ALONG, 5, 1), (ALONG, 5, 2),),
    ((ARRIVED, 1, 0), (ACROSS, 10, 1), (SEND_ALONG, 8, 0), (ALONG, 5, 3), (ACROSS, 4, 1), (ACROSS, 4, 2),
     (ACROSS, 4, 3), (ACROSS, 3, 2),),
    (),
    (),
    ((ALONG, 8, 1), (ACROSS, 3, 3),),
    ((ACROSS, 6, 3), (ACROSS, 6, 1), (ALONG, 8, 2), (SEND_ACROSS, 7, 0), (ACROSS, 5, 1), (ALONG, 7, 1),
     (SEND_ACROSS, 8, 0),),
    ((ACROSS, 5, 2),),
    ((ARRIVED, 2, 0), (ACROSS, 6, 2), (SEND_ALONG, 10, 0), (ALONG, 7, 3),),
    ((ALONG, 7, 2),),
    ((ACROSS, 8, 2), (ACROSS, 5, 0),),
    ((SEND_ACROSS, 9, 0), (ACROSS, 5, 3), (ALONG, 10, 2), (ALONG, 10, 3),),
    ((ACROSS, 8, 0), (ALONG, 8, 3), (ACROSS, 7, 3), (ACROSS, 7, 0), (ARRIVED, 3, 0),),
    ((ACROSS, 9, 1), (ACROSS, 9, 3), (ACROSS, 9, 0), (ACROSS, 7, 2), (ACROSS, 7, 1), (ACROSS, 9, 2), (ACROSS, 8, 1),),
    (),
    (),
    ((ACROSS, 10, 2), (ACROSS, 10, 3), (ACROSS, 8, 3),),
)


class Chunk:
    def __init__(self, index, weight, shard, part, parts, along, across_own, across):
        units = shard // TILE
        first, last = units * part // parts, units * (part + 1) // parts
        count = last - first
        least = (count + 1) // 2
        self.index, self.weight, self.shard = index, weight, shard
        self.offset, self.rows = first * TILE, count * TILE

        def share(tiles, most):
            return TILE * min(max(round(count * tiles / UNITS[index]), least), most)

        self.along = share(along, count)
        self.across_own = share(across_own, count)
        self.across = share(across, self.along // TILE)


def plain(chunks, n, seqs):
    counts = {0: seqs, 1: seqs + 2, 2: seqs, 3: seqs}
    segments = [[(name, chunk.index, 0) for chunk in chunks[HEAD:] for name in (SEND_ALONG, SEND_ACROSS)]]
    segments += [[] for _ in range(seqs)]
    for weight in range(5):
        for chunk in chunks:
            if chunk.weight == weight:
                for j in range(1, n):
                    segments[-1] += [(ALONG, chunk.index, j), (ACROSS, chunk.index, j - 1)]
                segments[-1].append((ACROSS, chunk.index, n - 1))
        if 1 <= weight <= 3:
            segments[-1].append((ARRIVED, weight, 0))
            segments += [[] for _ in range(counts[weight])]
    return segments


def dot(left, right):
    return jnp.dot(left, right, preferred_element_type=jnp.float32)


def layer_kernel(n, chunks, segments, *refs):
    x_in, pool_in, out_in, up_in, gate_in, down_in = refs[:6]
    small_in, xm, small = refs[6:14], refs[14], refs[15:23]
    poolb, outb, upb, gateb, downb, s_pool, s_out, s_up, s_gate, s_down = refs[23:33]
    keep, sent, recv, cn, lift, ss, ssr = refs[33:40]
    in_sem, zs, zr, ys, yr, xs, xr, ts, tr = refs[40:]
    mix_gain, pool_scale, out_scale, channel_gain, up_scale, gate_scale, conv_weight, down_scale = small
    buffers = (poolb, outb, upb, gateb, downb)

    rows, half = xm.shape
    width = 2 * half
    seqs = rows // LENGTH
    shards = 2 * n
    blocks, _, block = keep.shape
    hidden_width = lift.shape[1]
    group = poolb.shape[1]
    groups = half // group
    pool_rows = pool_in.shape[0]
    lane = pool_rows // groups

    r, f, core = lax.axis_index("rep"), lax.axis_index("fs"), lax.axis_index("tp")
    a, b = f // 2, f % 2

    def order(j):
        near = jnp.minimum(a, n - 1 - a)
        odd = j % 2
        way = jnp.where(a < n - 1 - a, 1, -1)
        paired = a + way * (1 - 2 * odd) * ((j + 1) // 2)
        return jnp.where(j <= 2 * near, paired, a + way * (j - near))

    def rows_of(chunk, shard, start, count):
        begin = pl.multiple_of(shard * chunk.shard + chunk.offset + start, TILE)
        return buffers[chunk.weight].at[pl.ds(begin, count)]

    def z_copy(chunk, s, target):
        part = rows_of(chunk, 2 * s + b, r * (chunk.rows - chunk.along), chunk.along)
        return pltpu.make_async_remote_copy(
            src_ref=part, dst_ref=part, send_sem=zs.at[chunk.index], recv_sem=zr.at[chunk.index, s],
            device_id={"fs": 2 * target + b}, device_id_type=MESH,
        )

    def y_copy(chunk, s, side, own):
        had = chunk.across_own if own else chunk.across
        part = rows_of(chunk, 2 * s + side, r * (chunk.rows - had), had)
        return pltpu.make_async_remote_copy(
            src_ref=part, dst_ref=part, send_sem=ys.at[chunk.index], recv_sem=yr.at[chunk.index, s],
            device_id={"fs": 2 * a + 1 - b}, device_id_type=MESH,
        )

    def x_copy(chunk, s, kind, end, own=False):
        had = chunk.along if kind == 0 else chunk.across_own if own else chunk.across
        part = rows_of(chunk, 2 * s + (1 - b if kind else b), end * had, chunk.rows - had)
        return pltpu.make_async_remote_copy(
            src_ref=part, dst_ref=part, send_sem=xs.at[chunk.index], recv_sem=xr.at[chunk.index, n * kind + s if chunk.weight == 4 else 0],
            device_id={"rep": 1 - r}, device_id_type=MESH,
        )

    def onward(s):
        target = jnp.where(s < a, a + 1, a - 1)
        return target, (target >= 0) & (target < n)

    def begin_along(chunk):
        @pl.when(a < n - 1)
        def _():
            z_copy(chunk, a, a + 1).start()

        @pl.when(a > 0)
        def _():
            z_copy(chunk, a, a - 1).start()

    def begin_across(chunk):
        y_copy(chunk, a, b, True).start()

    def z_event(chunk, j):
        s = order(j)
        target, valid = onward(s)
        z_copy(chunk, s, a).wait_recv()

        @pl.when(valid)
        def _():
            z_copy(chunk, s, target).start()

        y_copy(chunk, s, b, False).start()
        if chunk.rows > chunk.along:
            x_copy(chunk, s, 0, r).start()

    def y_event(chunk, j):
        s = order(j)
        own = j == 0
        y_copy(chunk, s, 1 - b, own).wait_recv()
        if chunk.rows > (chunk.across_own if own else chunk.across):
            x_copy(chunk, s, 1, r, own).start()

    def x_wait(chunk, j, kind, own=False):
        had = chunk.along if kind == 0 else chunk.across_own if own else chunk.across
        if chunk.rows > had:
            x_copy(chunk, order(j), kind, 1 - r, own).wait_recv()

    def bulk(chunk, sem, count):
        part = buffers[chunk.weight].at[pl.ds(0, count)]
        return pltpu.make_async_copy(part, part, sem)

    def swapped(chunk):
        return chunk.rows - chunk.across_own + (n - 1) * (2 * chunk.rows - chunk.along - chunk.across)

    def arrived(weights):
        for chunk in chunks:
            if chunk.weight in weights and swapped(chunk):
                bulk(chunk, xr.at[chunk.index, 0], swapped(chunk)).wait()

    inner = (a > 0) & (a < n - 1)

    def finish(chunk):
        @pl.when(inner)
        def _():
            bulk(chunk, zs.at[chunk.index], (n + 1) * chunk.along).wait()

        @pl.when(jnp.logical_not(inner))
        def _():
            bulk(chunk, zs.at[chunk.index], chunk.along).wait()

        bulk(chunk, ys.at[chunk.index], chunk.across_own + (n - 1) * chunk.across).wait()
        if swapped(chunk):
            bulk(chunk, xs.at[chunk.index], swapped(chunk)).wait()

    def events(segment):
        for name, index, j in segment:
            if name == SEND_ALONG:
                begin_along(chunks[index])
            elif name == SEND_ACROSS:
                begin_across(chunks[index])
            elif name == ALONG:
                z_event(chunks[index], j)
            elif name == ACROSS:
                y_event(chunks[index], j)
            else:
                arrived((0, 1) if index == 1 else (index,))

    def between(ends, middles):
        if ends == middles:
            events(ends)
            return

        @pl.when(jnp.logical_not(inner))
        def _():
            events(ends)

        @pl.when(inner)
        def _():
            events(middles)

    def stage(first, count, piece):
        def step(q, carry):
            piece(q)
            for i in range(count):
                if segments[0][first + i] or segments[1][first + i]:

                    @pl.when(q == i)
                    def _(i=i):
                        between(segments[0][first + i], segments[1][first + i])

            return carry

        lax.fori_loop(0, count, step, 0)

    def t_copy(kind, index, src, dst):
        return pltpu.make_async_remote_copy(
            src_ref=src, dst_ref=dst, send_sem=ts.at[kind, index], recv_sem=tr.at[kind, index],
            device_id={"tp": 1 - core}, device_id_type=MESH,
        )

    def span(q):
        return pl.ds(pl.multiple_of(q * LENGTH, LENGTH), LENGTH)

    def norm_copy(kind, q):
        return t_copy(2 * kind, q, ss.at[kind, span(q)], ssr.at[kind, span(q)])

    def mixer_copy(q):
        return t_copy(1, q, sent.at[:, span(q)], recv.at[:, span(q)])

    def cn_copy(q, side):
        return t_copy(3, q, cn.at[side, span(q)], cn.at[side, span(q)])

    def down_copy(index):
        return t_copy(4, index, sent.at[index], recv.at[index])

    def line(ref):
        return ref[...].astype(jnp.float32).reshape(1, -1)

    def sum_squares(kind, q):
        values = xm[span(q)].astype(jnp.float32)
        total = jnp.sum(values * values, axis=1, keepdims=True)
        ss[kind, span(q)] = jnp.broadcast_to(total, (LENGTH, ss.shape[2]))

    def inverse(kind, q):
        norm_copy(kind, q).wait_recv()
        total = ss[kind, span(q)][:, :1] + ssr[kind, span(q)][:, :1]
        return lax.rsqrt(total / width + EPS)

    def pool_piece(q):
        values = xm[span(q)].astype(jnp.float32)
        normed = (values * inverse(0, q) * line(mix_gain)).astype(jnp.bfloat16)
        at = lax.broadcasted_iota(jnp.int32, (LENGTH, LENGTH), 0)
        to = lax.broadcasted_iota(jnp.int32, (LENGTH, LENGTH), 1)
        for local in range(groups):
            reach = jnp.left_shift(jnp.int32(1), core * groups + local)
            lower = jnp.maximum(at - reach, 0)
            upper = jnp.minimum(at + reach, LENGTH)
            band = jnp.where((to >= lower) & (to < upper), 1.0, 0.0).astype(jnp.bfloat16)
            count = (upper[:, :1] - lower[:, :1]).astype(jnp.float32)
            part = normed[:, local * group : (local + 1) * group]
            pooled = dot(band, part) / count - part.astype(jnp.float32)
            cn[1 - core, span(q), local * group : (local + 1) * group] = pooled.astype(jnp.bfloat16)

    def mix_piece(q):
        grouped = []
        for local in range(groups):
            pooled = cn[1 - core, span(q), local * group : (local + 1) * group]
            linear = jnp.concatenate(
                [poolb[s * pool_rows + local * lane : s * pool_rows + (local + 1) * lane, :] for s in range(shards)], axis=0
            )
            product = lax.dot_general(pooled, linear, (((1,), (1,)), ((), ())), preferred_element_type=jnp.float32)
            grouped.append((product * pool_scale[local : local + 1, :]).astype(jnp.bfloat16))
        grouped = jnp.concatenate(grouped, axis=1)
        for target, side in ((sent, 1 - core), (keep, core)):

            def one(index, carry):
                start = pl.multiple_of((side * blocks + index) * half, TILE)
                target[index, span(q)] = dot(grouped, outb[pl.ds(start, half), :]).astype(jnp.bfloat16)
                return carry

            lax.fori_loop(0, blocks, one, 0)

    def both(q):
        return jnp.concatenate(
            [keep[i, span(q)].astype(jnp.float32) + recv[i, span(q)].astype(jnp.float32) for i in range(blocks)], axis=1
        )

    def middle_piece(q):
        copy = mixer_copy(q)
        copy.wait_recv()
        copy.wait_send()
        xm[span(q)] = (xm[span(q)].astype(jnp.float32) + both(q) * line(out_scale)).astype(jnp.bfloat16)
        sum_squares(1, q)

    def cn_piece(q):
        values = xm[span(q)].astype(jnp.float32)
        cn[core, span(q)] = (values * inverse(1, q) * line(channel_gain)).astype(jnp.bfloat16)

    def mixer_step(t):
        @pl.when(t >= 2)
        def _():
            cn_piece(t - 2)

        @pl.when((t >= 1) & (t <= seqs))
        def _():
            middle_piece(t - 1)
            norm_copy(1, t - 1).start()

        @pl.when(t < seqs)
        def _():
            mix_piece(t)
            mixer_copy(t).start()

        @pl.when(t >= 2)
        def _():
            cn_copy(t - 2, core).start()

    def wide(q, weight):
        return dot(cn[0, span(q)], weight[:half, :]) + dot(cn[1, span(q)], weight[half:, :])

    def lift_piece(q):
        cn_copy(q, 1 - core).wait_recv()
        lifted = (wide(q, upb) * line(up_scale)).astype(jnp.bfloat16).astype(jnp.float32)
        at = lax.broadcasted_iota(jnp.int32, (LENGTH, 1), 0)
        before = jnp.where(at == 0, 0.0, pltpu.roll(lifted, 1, 0))
        after = jnp.where(at == LENGTH - 1, 0.0, pltpu.roll(lifted, LENGTH - 1, 0))
        conv = conv_weight[0:1, :] * before + conv_weight[1:2, :] * lifted + conv_weight[2:3, :] * after
        lift[span(q)] = jax.nn.gelu(conv).astype(jnp.bfloat16)

    def hidden_piece(q):
        gated = wide(q, gateb) * line(gate_scale)
        lift[span(q)] = (lift[span(q)].astype(jnp.float32) * gated).astype(jnp.bfloat16)

    loads = [
        pltpu.make_async_copy(out_in, s_out, in_sem.at[0]),
        pltpu.make_async_copy(pool_in, s_pool, in_sem.at[1]),
        pltpu.make_async_copy(x_in, xm, in_sem.at[2]),
        pltpu.make_async_copy(up_in, s_up, in_sem.at[3]),
        pltpu.make_async_copy(gate_in, s_gate, in_sem.at[4]),
        pltpu.make_async_copy(down_in, s_down, in_sem.at[5]),
    ] + [pltpu.make_async_copy(src, dst, in_sem.at[6 + i]) for i, (src, dst) in enumerate(zip(small_in, small))]
    for load in loads:
        load.start()
    barrier = pltpu.get_barrier_semaphore()
    for peer in ({"rep": 1 - r}, {"fs": 2 * a + 1 - b}, {"tp": 1 - core}):
        pl.semaphore_signal(barrier, inc=1, device_id=peer, device_id_type=MESH)

    @pl.when(a > 0)
    def _():
        pl.semaphore_signal(barrier, inc=1, device_id={"fs": f - 2}, device_id_type=MESH)

    @pl.when(a < n - 1)
    def _():
        pl.semaphore_signal(barrier, inc=1, device_id={"fs": f + 2}, device_id_type=MESH)

    def settle(load, staged, full):
        loads[load].wait()
        count = staged.shape[0]
        full[pl.ds(pl.multiple_of(f * count, TILE), count), :] = staged[...].astype(jnp.bfloat16)

    settle(1, s_pool, poolb)
    settle(0, s_out, outb)
    ends = jnp.where(a > 0, 1, 0) + jnp.where(a < n - 1, 1, 0)
    pl.semaphore_wait(barrier, 3 + ends)

    for chunk in chunks[:HEAD]:
        begin_along(chunk)
        begin_across(chunk)
    settle(3, s_up, upb)
    for load in loads[2:3] + loads[6:]:
        load.wait()

    def first_sum(q, carry):
        sum_squares(0, q)
        return carry

    lax.fori_loop(0, seqs, first_sum, 0)

    def first_send(q, carry):
        norm_copy(0, q).start()
        return carry

    lax.fori_loop(0, seqs, first_send, 0)
    settle(4, s_gate, gateb)
    settle(5, s_down, downb)
    between(segments[0][0], segments[1][0])

    stage(1, seqs, pool_piece)
    stage(1 + seqs, seqs + 2, mixer_step)
    stage(3 + 2 * seqs, seqs, lift_piece)
    stage(3 + 3 * seqs, seqs, hidden_piece)
    down_c = [chunk for chunk in chunks if chunk.weight == 4]
    for chunk in chunks:
        if chunk.weight < 4:
            finish(chunk)

    shard_rows = s_down.shape[0]

    def down_step(i, carry):
        j, kind = i // 2, i % 2
        s = order(j)

        @pl.when((kind == 1) & (j == 0))
        def _():
            for chunk in down_c:
                x_wait(chunk, 0, 1, True)

        @pl.when((kind == 1) & (j > 0))
        def _():
            for chunk in down_c:
                x_wait(chunk, j, 1)

        @pl.when((kind == 0) & (j > 0))
        def _():
            for chunk in down_c:
                x_wait(chunk, j, 0)

        shard = 2 * s + (b + kind) % 2
        start = pl.multiple_of(shard * shard_rows, TILE)
        side, index = shard // blocks, shard % blocks
        product = dot(lift[...], downb[pl.ds(start, shard_rows), :]).astype(jnp.bfloat16)

        @pl.when(side == core)
        def _():
            keep[index] = product

        @pl.when(side != core)
        def _():
            sent[index] = product
            down_copy(index).start()

        return carry

    lax.fori_loop(0, shards, down_step, 0)

    def down_wait(index, carry):
        down_copy(index).wait_recv()
        return carry

    lax.fori_loop(0, blocks, down_wait, 0)

    def last(q, carry):
        xm[span(q)] = (xm[span(q)].astype(jnp.float32) + both(q) * line(down_scale)).astype(jnp.bfloat16)
        return carry

    lax.fori_loop(0, seqs, last, 0)

    for chunk in down_c:
        finish(chunk)

    def sends(q, carry):
        norm_copy(0, q).wait_send()
        norm_copy(1, q).wait_send()
        cn_copy(q, core).wait_send()
        return carry

    lax.fori_loop(0, seqs, sends, 0)

    def down_sends(index, carry):
        down_copy(index).wait_send()
        return carry

    lax.fori_loop(0, blocks, down_sends, 0)


def per_device(
    shards,
    layer_in,
    mix_gain,
    pool_weight,
    pool_scale,
    out_weight,
    out_scale,
    channel_gain,
    up_weight,
    up_scale,
    gate_weight,
    gate_scale,
    conv_weight,
    down_weight,
    down_scale,
):
    rows, half = layer_in.shape
    n = shards // 2
    hidden_width = up_weight.shape[1]
    groups, group, lane = pool_weight.shape
    block = out_weight.shape[1]
    blocks = half // block
    seqs = rows // LENGTH
    pool_rows = jnp.transpose(pool_weight, (0, 2, 1)).reshape(groups * lane, group)
    small = (
        mix_gain,
        pool_scale,
        out_scale.reshape(1, -1),
        channel_gain,
        up_scale,
        gate_scale,
        conv_weight,
        down_scale.reshape(1, -1),
    )
    heights = (groups * lane, half, up_weight.shape[0], gate_weight.shape[0], hidden_width)
    chunks = [Chunk(i, entry[0], heights[entry[0]], *entry[1:]) for i, entry in enumerate(PLAN)]
    segments = (ENDS, MIDDLES) if n == 4 and seqs == 4 else (plain(chunks, n, seqs),) * 2
    count = len(chunks)
    bf16, f32 = jnp.bfloat16, jnp.float32
    dma = pltpu.SemaphoreType.DMA
    return pl.pallas_call(
        functools.partial(layer_kernel, n, chunks, segments),
        out_shape=pltpu.VMEM((rows, half), bf16),
        in_specs=[pl.BlockSpec(memory_space=pl.ANY)] * (6 + len(small)),
        out_specs=pl.BlockSpec(memory_space=pltpu.VMEM),
        scratch_shapes=[pltpu.VMEM(v.shape, v.dtype) for v in small]
        + [
            pltpu.VMEM((shards * groups * lane, group), bf16),
            pltpu.VMEM((shards * half, block), bf16),
            pltpu.VMEM((shards * up_weight.shape[0], hidden_width), bf16),
            pltpu.VMEM((shards * gate_weight.shape[0], hidden_width), bf16),
            pltpu.VMEM((shards * hidden_width, block), bf16),
            pltpu.VMEM(pool_rows.shape, f32),
            pltpu.VMEM(out_weight.shape, f32),
            pltpu.VMEM(up_weight.shape, f32),
            pltpu.VMEM(gate_weight.shape, f32),
            pltpu.VMEM(down_weight.shape, f32),
            pltpu.VMEM((blocks, rows, block), bf16),
            pltpu.VMEM((blocks, rows, block), bf16),
            pltpu.VMEM((blocks, rows, block), bf16),
            pltpu.VMEM((2, rows, half), bf16),
            pltpu.VMEM((rows, hidden_width), bf16),
            pltpu.VMEM((2, rows, 128), f32),
            pltpu.VMEM((2, rows, 128), f32),
            dma((6 + len(small),)),
            dma((count,)),
            dma((count, n)),
            dma((count,)),
            dma((count, n)),
            dma((count,)),
            dma((count, 2 * n)),
            dma((5, max(seqs, blocks))),
            dma((5, max(seqs, blocks))),
        ],
        compiler_params=pltpu.CompilerParams(
            collective_id=0, has_side_effects=True, vmem_limit_bytes=62_000_000
        ),
        name="layer",
    )(layer_in, pool_rows, out_weight, up_weight, gate_weight, down_weight, *small)


def solution(mesh):
    placed = (
        P(("rep", "fs"), "tp"),
        P("tp"),
        P("tp", None, "fs"),
        P("tp", None),
        P("tp", "fs"),
        P("tp"),
        P("tp"),
        P("fs", "tp"),
        P("tp"),
        P("fs", "tp"),
        P("tp"),
        P(None, "tp"),
        P("tp", "fs"),
        P("tp"),
    )
    body = functools.partial(per_device, mesh.shape["fs"])
    return jax.shard_map(
        body, mesh=mesh, in_specs=placed, out_specs=P(("rep", "fs"), "tp"), check_vma=False
    )
```

```python
import functools

import jax
import jax.numpy as jnp
from jax import lax
from jax.experimental import pallas as pl
from jax.experimental.pallas import tpu as pltpu
from jax.sharding import PartitionSpec as P

LENGTH = 256
EPS = 1e-06
TILE = 16
MESH = pl.DeviceIdType.MESH

PLAN = (
    (0, 0, 8, 4, 4, 4),
    (1, 0, 32, 17, 16, 17),
    (1, 32, 64, 19, 20, 17),
    (2, 0, 8, 4, 4, 4),
    (2, 8, 16, 4, 6, 4),
    (3, 0, 8, 8, 4, 7),
    (3, 8, 16, 8, 5, 4),
    (4, 0, 22, 22, 12, 15),
    (4, 22, 44, 21, 14, 11),
    (4, 44, 66, 21, 11, 12),
    (4, 66, 88, 22, 16, 22),
)
UNITS = (8, 64, 16, 16, 88)
HEAD = 2
SEND_ALONG, SEND_ACROSS, ALONG, ACROSS, ARRIVED = range(5)

ENDS = (
    ((SEND_ALONG, 10, 0), (SEND_ACROSS, 3, 0), (ALONG, 0, 1), (ACROSS, 0, 0), (SEND_ACROSS, 8, 0),),
    ((ACROSS, 1, 0), (ALONG, 1, 1), (SEND_ALONG, 2, 0),),
    ((ALONG, 2, 1), (ACROSS, 3, 0), (SEND_ACROSS, 2, 0), (SEND_ALONG, 4, 0), (ALONG, 4, 1), (SEND_ALONG, 3, 0),
     (ALONG, 1, 2), (SEND_ALONG, 9, 0), (ACROSS, 0, 1), (ALONG, 3, 1), (ACROSS, 1, 1), (ALONG, 0, 3),
     (SEND_ALONG, 6, 0), (ACROSS, 2, 1), (SEND_ALONG, 7, 0), (ALONG, 0, 2), (ACROSS, 1, 2),),
    ((ACROSS, 4, 1), (SEND_ACROSS, 7, 0), (ACROSS, 0, 3), (ALONG, 2, 3), (SEND_ALONG, 8, 0), (SEND_ALONG, 5, 0),
     (ACROSS, 2, 0), (SEND_ACROSS, 5, 0),),
    ((ALONG, 2, 2), (ACROSS, 5, 0), (ACROSS, 3, 1), (ACROSS, 2, 3), (SEND_ACROSS, 9, 0), (SEND_ACROSS, 4, 0),
     (ALONG, 4, 3), (ALONG, 3, 3), (ALONG, 1, 3), (ALONG, 4, 2), (ACROSS, 0, 2), (SEND_ACROSS, 6, 0), (ACROSS, 1, 3),
     (ACROSS, 4, 0), (ACROSS, 2, 2), (ALONG, 3, 2), (ALONG, 5, 1), (ACROSS, 9, 0), (ACROSS, 3, 2), (ALONG, 6, 1),
     (ACROSS, 5, 1), (SEND_ACROSS, 10, 0), (ARRIVED, 1, 0), (ALONG, 6, 3), (ALONG, 9, 1), (ACROSS, 4, 3),),
    ((ALONG, 6, 2), (ALONG, 8, 1), (ALONG, 5, 3), (ACROSS, 6, 1), (ACROSS, 4, 2), (ACROSS, 3, 3),),
    (),
    ((ALONG, 5, 2),),
    ((ACROSS, 6, 2),),
    ((ALONG, 7, 1), (ACROSS, 6, 0),),
    ((ACROSS, 6, 3), (ALONG, 9, 2), (ARRIVED, 2, 0),),
    (),
    ((ACROSS, 5, 2), (ALONG, 10, 1),),
    ((ALONG, 8, 3), (ACROSS, 5, 3), (ACROSS, 9, 2), (ACROSS, 8, 1), (ACROSS, 7, 0), (ACROSS, 8, 0), (ALONG, 8, 2),),
    ((ACROSS, 7, 1), (ACROSS, 10, 0), (ALONG, 7, 2), (ARRIVED, 3, 0),),
    ((ALONG, 9, 3), (ACROSS, 9, 1),),
    (),
    ((ACROSS, 8, 3), (ACROSS, 10, 1), (ACROSS, 8, 2), (ALONG, 10, 2),),
    ((ACROSS, 7, 2), (ALONG, 7, 3),),
    (),
    (),
    ((ACROSS, 10, 2), (ALONG, 10, 3), (ACROSS, 9, 3),),
    ((ACROSS, 7, 3),),
    (),
    (),
    ((ACROSS, 10, 3),),
    (),
)
MIDDLES = (
    ((SEND_ALONG, 2, 0), (SEND_ALONG, 4, 0), (ACROSS, 0, 0), (ALONG, 0, 1), (ALONG, 0, 2), (ALONG, 1, 2),
     (SEND_ACROSS, 9, 0), (SEND_ALONG, 3, 0), (ACROSS, 1, 0),),
    ((ALONG, 1, 1), (ALONG, 2, 1), (ALONG, 4, 1), (ACROSS, 1, 1), (SEND_ALONG, 8, 0), (ALONG, 0, 3), (ALONG, 1, 3),
     (ALONG, 2, 2), (ACROSS, 2, 1), (ALONG, 2, 3), (ALONG, 3, 2), (ALONG, 3, 1), (SEND_ALONG, 7, 0), (ALONG, 6, 1),
     (SEND_ACROSS, 6, 0), (ACROSS, 0, 1), (SEND_ACROSS, 8, 0), (ALONG, 3, 3), (ALONG, 4, 3), (ACROSS, 2, 2),
     (ALONG, 4, 2), (ACROSS, 6, 0), (SEND_ALONG, 5, 0), (SEND_ACROSS, 2, 0), (ACROSS, 6, 1), (ALONG, 5, 1),
     (ACROSS, 2, 3), (SEND_ACROSS, 5, 0), (SEND_ACROSS, 3, 0), (ALONG, 6, 3), (SEND_ALONG, 6, 0),),
    (),
    ((ACROSS, 0, 2), (ACROSS, 0, 3), (ACROSS, 1, 3), (ACROSS, 4, 3), (ALONG, 9, 1), (SEND_ALONG, 9, 0),
     (SEND_ACROSS, 4, 0), (ACROSS, 4, 1), (ACROSS, 2, 0), (SEND_ACROSS, 7, 0),),
    ((ALONG, 6, 2), (ACROSS, 1, 2), (ACROSS, 3, 3), (ACROSS, 5, 0), (ALONG, 5, 3), (SEND_ACROSS, 10, 0),
     (ALONG, 5, 2), (ALONG, 10, 1), (ARRIVED, 1, 0), (ACROSS, 3, 1), (ACROSS, 3, 2), (ACROSS, 3, 0), (ACROSS, 4, 2),),
    (),
    ((ALONG, 8, 2),),
    ((ALONG, 8, 1),),
    ((ACROSS, 4, 0), (ACROSS, 6, 3), (ALONG, 9, 2),),
    ((SEND_ALONG, 10, 0), (ALONG, 7, 1),),
    ((ALONG, 8, 3), (ACROSS, 5, 1), (ACROSS, 5, 2), (ARRIVED, 2, 0), (ACROSS, 6, 2), (ACROSS, 10, 0), (ALONG, 7, 2),
     (ALONG, 9, 3), (ACROSS, 9, 0), (ALONG, 10, 2),),
    ((ACROSS, 5, 3), (ACROSS, 7, 0),),
    (),
    ((ACROSS, 8, 1),),
    ((ACROSS, 9, 1), (ALONG, 7, 3), (ARRIVED, 3, 0), (ACROSS, 8, 0),),
    ((ACROSS, 7, 1),),
    ((ACROSS, 8, 2), (ACROSS, 9, 2), (ALONG, 10, 3),),
    (),
    ((ACROSS, 8, 3), (ACROSS, 10, 1),),
    ((ACROSS, 7, 2), (ACROSS, 9, 3),),
    (),
    (),
    ((ACROSS, 7, 3), (ACROSS, 10, 2),),
    (),
    (),
    ((ACROSS, 10, 3),),
    (),
)


class Chunk:
    def __init__(self, index, weight, shard, first, last, along, across_own, across):
        tiles = shard // TILE
        begin, end = tiles * first // UNITS[weight], tiles * last // UNITS[weight]
        count = end - begin
        least = (count + 1) // 2
        self.index, self.weight, self.shard = index, weight, shard
        self.offset, self.rows = begin * TILE, count * TILE

        def share(part, most):
            return TILE * min(max(round(count * part / (last - first)), least), most)

        self.along = share(along, count)
        self.across_own = share(across_own, count)
        self.across = share(across, self.along // TILE)


def plain(chunks, n, seqs):
    counts = {0: seqs, 1: seqs + 2, 2: seqs, 3: seqs}
    segments = [[(name, chunk.index, 0) for chunk in chunks[HEAD:] for name in (SEND_ALONG, SEND_ACROSS)]]
    segments += [[] for _ in range(seqs)]
    for weight in range(5):
        for chunk in chunks:
            if chunk.weight == weight:
                for j in range(1, n):
                    segments[-1] += [(ALONG, chunk.index, j), (ACROSS, chunk.index, j - 1)]
                segments[-1].append((ACROSS, chunk.index, n - 1))
        if 1 <= weight <= 3:
            segments[-1].append((ARRIVED, weight, 0))
            segments += [[] for _ in range(counts[weight])]
    return segments


def dot(left, right):
    return jnp.dot(left, right, preferred_element_type=jnp.float32)


def layer_kernel(n, chunks, segments, *refs):
    x_in, pool_in, out_in, up_in, gate_in, down_in = refs[:6]
    small_in, xm, small = refs[6:14], refs[14], refs[15:23]
    poolb, outb, upb, gateb, downb, s_pool, s_out, s_up, s_gate, s_down = refs[23:33]
    keep, sent, recv, cn, lift, ss, ssr = refs[33:40]
    in_sem, zs, zr, ys, yr, xs, xr, ts, tr = refs[40:]
    mix_gain, pool_scale, out_scale, channel_gain, up_scale, gate_scale, conv_weight, down_scale = small
    buffers = (poolb, outb, upb, gateb, downb)

    rows, half = xm.shape
    width = 2 * half
    seqs = rows // LENGTH
    shards = 2 * n
    blocks, _, block = keep.shape
    hidden_width = lift.shape[1]
    group = poolb.shape[1]
    groups = half // group
    pool_rows = pool_in.shape[0]
    lane = pool_rows // groups

    r, f, core = lax.axis_index("rep"), lax.axis_index("fs"), lax.axis_index("tp")
    a, b = f // 2, f % 2

    def order(j):
        near = jnp.minimum(a, n - 1 - a)
        odd = j % 2
        way = jnp.where(a < n - 1 - a, 1, -1)
        paired = a + way * (1 - 2 * odd) * ((j + 1) // 2)
        return jnp.where(j <= 2 * near, paired, a + way * (j - near))

    def rows_of(chunk, shard, start, count):
        begin = pl.multiple_of(shard * chunk.shard + chunk.offset + start, TILE)
        return buffers[chunk.weight].at[pl.ds(begin, count)]

    def z_copy(chunk, s, target):
        part = rows_of(chunk, 2 * s + b, r * (chunk.rows - chunk.along), chunk.along)
        return pltpu.make_async_remote_copy(
            src_ref=part, dst_ref=part, send_sem=zs.at[chunk.index], recv_sem=zr.at[chunk.index, s],
            device_id={"fs": 2 * target + b}, device_id_type=MESH,
        )

    def y_copy(chunk, s, side, own):
        had = chunk.across_own if own else chunk.across
        part = rows_of(chunk, 2 * s + side, r * (chunk.rows - had), had)
        return pltpu.make_async_remote_copy(
            src_ref=part, dst_ref=part, send_sem=ys.at[chunk.index], recv_sem=yr.at[chunk.index, s],
            device_id={"fs": 2 * a + 1 - b}, device_id_type=MESH,
        )

    def x_copy(chunk, s, kind, end, own=False):
        had = chunk.along if kind == 0 else chunk.across_own if own else chunk.across
        part = rows_of(chunk, 2 * s + (1 - b if kind else b), end * had, chunk.rows - had)
        return pltpu.make_async_remote_copy(
            src_ref=part, dst_ref=part, send_sem=xs.at[chunk.index], recv_sem=xr.at[chunk.index, n * kind + s if chunk.weight == 4 else 0],
            device_id={"rep": 1 - r}, device_id_type=MESH,
        )

    def onward(s):
        target = jnp.where(s < a, a + 1, a - 1)
        return target, (target >= 0) & (target < n)

    def begin_along(chunk):
        @pl.when(a < n - 1)
        def _():
            z_copy(chunk, a, a + 1).start()

        @pl.when(a > 0)
        def _():
            z_copy(chunk, a, a - 1).start()

    def begin_across(chunk):
        y_copy(chunk, a, b, True).start()

    def z_event(chunk, j):
        s = order(j)
        target, valid = onward(s)
        z_copy(chunk, s, a).wait_recv()

        @pl.when(valid)
        def _():
            z_copy(chunk, s, target).start()

        y_copy(chunk, s, b, False).start()
        if chunk.rows > chunk.along:
            x_copy(chunk, s, 0, r).start()

    def y_event(chunk, j):
        s = order(j)
        own = j == 0
        y_copy(chunk, s, 1 - b, own).wait_recv()
        if chunk.rows > (chunk.across_own if own else chunk.across):
            x_copy(chunk, s, 1, r, own).start()

    def x_wait(chunk, j, kind, own=False):
        had = chunk.along if kind == 0 else chunk.across_own if own else chunk.across
        if chunk.rows > had:
            x_copy(chunk, order(j), kind, 1 - r, own).wait_recv()

    def bulk(chunk, sem, count):
        part = buffers[chunk.weight].at[pl.ds(0, count)]
        return pltpu.make_async_copy(part, part, sem)

    def swapped(chunk):
        return chunk.rows - chunk.across_own + (n - 1) * (2 * chunk.rows - chunk.along - chunk.across)

    def arrived(weights):
        for chunk in chunks:
            if chunk.weight in weights and swapped(chunk):
                bulk(chunk, xr.at[chunk.index, 0], swapped(chunk)).wait()

    inner = (a > 0) & (a < n - 1)

    def finish(chunk):
        @pl.when(inner)
        def _():
            bulk(chunk, zs.at[chunk.index], (n + 1) * chunk.along).wait()

        @pl.when(jnp.logical_not(inner))
        def _():
            bulk(chunk, zs.at[chunk.index], chunk.along).wait()

        bulk(chunk, ys.at[chunk.index], chunk.across_own + (n - 1) * chunk.across).wait()
        if swapped(chunk):
            bulk(chunk, xs.at[chunk.index], swapped(chunk)).wait()

    def events(segment):
        for name, index, j in segment:
            if name == SEND_ALONG:
                begin_along(chunks[index])
            elif name == SEND_ACROSS:
                begin_across(chunks[index])
            elif name == ALONG:
                z_event(chunks[index], j)
            elif name == ACROSS:
                y_event(chunks[index], j)
            else:
                arrived((0, 1) if index == 1 else (index,))

    def between(ends, middles):
        if ends == middles:
            events(ends)
            return

        @pl.when(jnp.logical_not(inner))
        def _():
            events(ends)

        @pl.when(inner)
        def _():
            events(middles)

    def stage(first, count, piece):
        def step(q, carry):
            piece(q)
            for i in range(count):
                if first + i < len(segments[0]) and (segments[0][first + i] or segments[1][first + i]):

                    @pl.when(q == i)
                    def _(i=i):
                        between(segments[0][first + i], segments[1][first + i])

            return carry

        lax.fori_loop(0, count, step, 0)

    def t_copy(kind, index, src, dst):
        return pltpu.make_async_remote_copy(
            src_ref=src, dst_ref=dst, send_sem=ts.at[kind, index], recv_sem=tr.at[kind, index],
            device_id={"tp": 1 - core}, device_id_type=MESH,
        )

    def span(q):
        return pl.ds(pl.multiple_of(q * LENGTH, LENGTH), LENGTH)

    def norm_copy(kind, q):
        return t_copy(2 * kind, q, ss.at[kind, span(q)], ssr.at[kind, span(q)])

    def mixer_copy(q):
        return t_copy(1, q, sent.at[:, span(q)], recv.at[:, span(q)])

    def cn_copy(q, side):
        return t_copy(3, q, cn.at[side, span(q)], cn.at[side, span(q)])

    def down_copy(index):
        return t_copy(4, index, sent.at[index], recv.at[index])

    def line(ref):
        return ref[...].astype(jnp.float32).reshape(1, -1)

    def sum_squares(kind, q):
        values = xm[span(q)].astype(jnp.float32)
        total = jnp.sum(values * values, axis=1, keepdims=True)
        ss[kind, span(q)] = jnp.broadcast_to(total, (LENGTH, ss.shape[2]))

    def inverse(kind, q):
        norm_copy(kind, q).wait_recv()
        total = ss[kind, span(q)][:, :1] + ssr[kind, span(q)][:, :1]
        return lax.rsqrt(total / width + EPS)

    def pool_piece(q):
        values = xm[span(q)].astype(jnp.float32)
        normed = (values * inverse(0, q) * line(mix_gain)).astype(jnp.bfloat16)
        at = lax.broadcasted_iota(jnp.int32, (LENGTH, LENGTH), 0)
        to = lax.broadcasted_iota(jnp.int32, (LENGTH, LENGTH), 1)
        for local in range(groups):
            reach = jnp.left_shift(jnp.int32(1), core * groups + local)
            lower = jnp.maximum(at - reach, 0)
            upper = jnp.minimum(at + reach, LENGTH)
            band = jnp.where((to >= lower) & (to < upper), 1.0, 0.0).astype(jnp.bfloat16)
            count = (upper[:, :1] - lower[:, :1]).astype(jnp.float32)
            part = normed[:, local * group : (local + 1) * group]
            pooled = dot(band, part) / count - part.astype(jnp.float32)
            cn[1 - core, span(q), local * group : (local + 1) * group] = pooled.astype(jnp.bfloat16)

    def mix_piece(q):
        grouped = []
        for local in range(groups):
            pooled = cn[1 - core, span(q), local * group : (local + 1) * group]
            linear = jnp.concatenate(
                [poolb[s * pool_rows + local * lane : s * pool_rows + (local + 1) * lane, :] for s in range(shards)], axis=0
            )
            product = lax.dot_general(pooled, linear, (((1,), (1,)), ((), ())), preferred_element_type=jnp.float32)
            grouped.append((product * pool_scale[local : local + 1, :]).astype(jnp.bfloat16))
        grouped = jnp.concatenate(grouped, axis=1)
        for target, side in ((sent, 1 - core), (keep, core)):

            def one(index, carry):
                start = pl.multiple_of((side * blocks + index) * half, TILE)
                target[index, span(q)] = dot(grouped, outb[pl.ds(start, half), :]).astype(jnp.bfloat16)
                return carry

            lax.fori_loop(0, blocks, one, 0)

    def both(q):
        return jnp.concatenate(
            [keep[i, span(q)].astype(jnp.float32) + recv[i, span(q)].astype(jnp.float32) for i in range(blocks)], axis=1
        )

    def middle_piece(q):
        copy = mixer_copy(q)
        copy.wait_recv()
        copy.wait_send()
        xm[span(q)] = (xm[span(q)].astype(jnp.float32) + both(q) * line(out_scale)).astype(jnp.bfloat16)
        sum_squares(1, q)

    def cn_piece(q):
        values = xm[span(q)].astype(jnp.float32)
        cn[core, span(q)] = (values * inverse(1, q) * line(channel_gain)).astype(jnp.bfloat16)

    def mixer_step(t):
        @pl.when(t >= 2)
        def _():
            cn_piece(t - 2)

        @pl.when((t >= 1) & (t <= seqs))
        def _():
            middle_piece(t - 1)
            norm_copy(1, t - 1).start()

        @pl.when(t < seqs)
        def _():
            mix_piece(t)
            mixer_copy(t).start()

        @pl.when(t >= 2)
        def _():
            cn_copy(t - 2, core).start()

    def wide(q, weight):
        return dot(cn[0, span(q)], weight[:half, :]) + dot(cn[1, span(q)], weight[half:, :])

    def lift_piece(q):
        cn_copy(q, 1 - core).wait_recv()
        lifted = (wide(q, upb) * line(up_scale)).astype(jnp.bfloat16).astype(jnp.float32)
        at = lax.broadcasted_iota(jnp.int32, (LENGTH, 1), 0)
        before = jnp.where(at == 0, 0.0, pltpu.roll(lifted, 1, 0))
        after = jnp.where(at == LENGTH - 1, 0.0, pltpu.roll(lifted, LENGTH - 1, 0))
        conv = conv_weight[0:1, :] * before + conv_weight[1:2, :] * lifted + conv_weight[2:3, :] * after
        lift[span(q)] = jax.nn.gelu(conv).astype(jnp.bfloat16)

    def hidden_piece(q):
        gated = wide(q, gateb) * line(gate_scale)
        lift[span(q)] = (lift[span(q)].astype(jnp.float32) * gated).astype(jnp.bfloat16)

    loads = [
        pltpu.make_async_copy(out_in, s_out, in_sem.at[0]),
        pltpu.make_async_copy(pool_in, s_pool, in_sem.at[1]),
        pltpu.make_async_copy(x_in, xm, in_sem.at[2]),
        pltpu.make_async_copy(up_in, s_up, in_sem.at[3]),
        pltpu.make_async_copy(gate_in, s_gate, in_sem.at[4]),
        pltpu.make_async_copy(down_in, s_down, in_sem.at[5]),
    ] + [pltpu.make_async_copy(src, dst, in_sem.at[6 + i]) for i, (src, dst) in enumerate(zip(small_in, small))]
    for load in loads:
        load.start()
    barrier = pltpu.get_barrier_semaphore()
    for peer in ({"rep": 1 - r}, {"fs": 2 * a + 1 - b}, {"tp": 1 - core}):
        pl.semaphore_signal(barrier, inc=1, device_id=peer, device_id_type=MESH)

    @pl.when(a > 0)
    def _():
        pl.semaphore_signal(barrier, inc=1, device_id={"fs": f - 2}, device_id_type=MESH)

    @pl.when(a < n - 1)
    def _():
        pl.semaphore_signal(barrier, inc=1, device_id={"fs": f + 2}, device_id_type=MESH)

    def settle(load, staged, full):
        loads[load].wait()
        count = staged.shape[0]
        full[pl.ds(pl.multiple_of(f * count, TILE), count), :] = staged[...].astype(jnp.bfloat16)

    settle(1, s_pool, poolb)
    settle(0, s_out, outb)
    ends = jnp.where(a > 0, 1, 0) + jnp.where(a < n - 1, 1, 0)
    pl.semaphore_wait(barrier, 3 + ends)

    for chunk in chunks[:HEAD]:
        begin_along(chunk)
        begin_across(chunk)
    settle(3, s_up, upb)
    for load in loads[2:3] + loads[6:]:
        load.wait()

    def first_sum(q, carry):
        sum_squares(0, q)
        return carry

    lax.fori_loop(0, seqs, first_sum, 0)

    def first_send(q, carry):
        norm_copy(0, q).start()
        return carry

    lax.fori_loop(0, seqs, first_send, 0)
    settle(4, s_gate, gateb)
    settle(5, s_down, downb)
    between(segments[0][0], segments[1][0])

    stage(1, seqs, pool_piece)
    stage(1 + seqs, seqs + 2, mixer_step)
    stage(3 + 2 * seqs, seqs, lift_piece)
    stage(3 + 3 * seqs, seqs, hidden_piece)
    down_c = [chunk for chunk in chunks if chunk.weight == 4]
    shard_rows = s_down.shape[0]

    def place(i):
        shard = 2 * order(i // 2) + (b + i) % 2
        return shard, shard // blocks, shard % blocks

    def settle_block(i):
        _, side, index = place(i)
        for k in range(blocks):

            @pl.when((side == core) & (index == k))
            def _(k=k):
                down_copy(k).wait_recv()
                columns = slice(k * block, (k + 1) * block)
                scale = down_scale[:, columns]

                def part(q, carry):
                    added = keep[k, span(q)].astype(jnp.float32) + recv[k, span(q)].astype(jnp.float32)
                    xm[span(q), columns] = (xm[span(q), columns].astype(jnp.float32) + added * scale).astype(jnp.bfloat16)
                    return carry

                lax.fori_loop(0, seqs, part, 0)

    def down_step(i):
        j, kind = i // 2, i % 2

        @pl.when(i >= 2)
        def _():
            settle_block(i - 2)

        @pl.when((kind == 1) & (j == 0))
        def _():
            for chunk in down_c:
                x_wait(chunk, 0, 1, True)

        @pl.when((kind == 1) & (j > 0) & (j < n))
        def _():
            for chunk in down_c:
                x_wait(chunk, j, 1)

        @pl.when((kind == 0) & (j > 0) & (j < n))
        def _():
            for chunk in down_c:
                x_wait(chunk, j, 0)

        @pl.when(j < n)
        def _():
            shard, side, index = place(i)
            start = pl.multiple_of(shard * shard_rows, TILE)
            product = dot(lift[...], downb[pl.ds(start, shard_rows), :]).astype(jnp.bfloat16)

            @pl.when(side == core)
            def _():
                keep[index] = product

            @pl.when(side != core)
            def _():
                sent[index] = product
                down_copy(index).start()

        @pl.when(i == shards)
        def _():
            for chunk in chunks:
                if chunk.weight < 4:
                    finish(chunk)

    stage(3 + 4 * seqs, shards + 2, down_step)

    for chunk in down_c:
        finish(chunk)

    def sends(q, carry):
        norm_copy(0, q).wait_send()
        norm_copy(1, q).wait_send()
        cn_copy(q, core).wait_send()
        return carry

    lax.fori_loop(0, seqs, sends, 0)

    def down_sends(index, carry):
        down_copy(index).wait_send()
        return carry

    lax.fori_loop(0, blocks, down_sends, 0)


def per_device(
    shards,
    layer_in,
    mix_gain,
    pool_weight,
    pool_scale,
    out_weight,
    out_scale,
    channel_gain,
    up_weight,
    up_scale,
    gate_weight,
    gate_scale,
    conv_weight,
    down_weight,
    down_scale,
):
    rows, half = layer_in.shape
    n = shards // 2
    hidden_width = up_weight.shape[1]
    groups, group, lane = pool_weight.shape
    block = out_weight.shape[1]
    blocks = half // block
    seqs = rows // LENGTH
    pool_rows = jnp.transpose(pool_weight, (0, 2, 1)).reshape(groups * lane, group)
    small = (
        mix_gain,
        pool_scale,
        out_scale.reshape(1, -1),
        channel_gain,
        up_scale,
        gate_scale,
        conv_weight,
        down_scale.reshape(1, -1),
    )
    heights = (groups * lane, half, up_weight.shape[0], gate_weight.shape[0], hidden_width)
    chunks = [Chunk(i, entry[0], heights[entry[0]], *entry[1:]) for i, entry in enumerate(PLAN)]
    segments = (ENDS, MIDDLES) if n == 4 and seqs == 4 else (plain(chunks, n, seqs),) * 2
    count = len(chunks)
    bf16, f32 = jnp.bfloat16, jnp.float32
    dma = pltpu.SemaphoreType.DMA
    return pl.pallas_call(
        functools.partial(layer_kernel, n, chunks, segments),
        out_shape=pltpu.VMEM((rows, half), bf16),
        in_specs=[pl.BlockSpec(memory_space=pl.ANY)] * (6 + len(small)),
        out_specs=pl.BlockSpec(memory_space=pltpu.VMEM),
        scratch_shapes=[pltpu.VMEM(v.shape, v.dtype) for v in small]
        + [
            pltpu.VMEM((shards * groups * lane, group), bf16),
            pltpu.VMEM((shards * half, block), bf16),
            pltpu.VMEM((shards * up_weight.shape[0], hidden_width), bf16),
            pltpu.VMEM((shards * gate_weight.shape[0], hidden_width), bf16),
            pltpu.VMEM((shards * hidden_width, block), bf16),
            pltpu.VMEM(pool_rows.shape, f32),
            pltpu.VMEM(out_weight.shape, f32),
            pltpu.VMEM(up_weight.shape, f32),
            pltpu.VMEM(gate_weight.shape, f32),
            pltpu.VMEM(down_weight.shape, f32),
            pltpu.VMEM((blocks, rows, block), bf16),
            pltpu.VMEM((blocks, rows, block), bf16),
            pltpu.VMEM((blocks, rows, block), bf16),
            pltpu.VMEM((2, rows, half), bf16),
            pltpu.VMEM((rows, hidden_width), bf16),
            pltpu.VMEM((2, rows, 128), f32),
            pltpu.VMEM((2, rows, 128), f32),
            dma((6 + len(small),)),
            dma((count,)),
            dma((count, n)),
            dma((count,)),
            dma((count, n)),
            dma((count,)),
            dma((count, 2 * n)),
            dma((5, max(seqs, blocks))),
            dma((5, max(seqs, blocks))),
        ],
        compiler_params=pltpu.CompilerParams(
            collective_id=0, has_side_effects=True, vmem_limit_bytes=62_000_000
        ),
        name="layer",
    )(layer_in, pool_rows, out_weight, up_weight, gate_weight, down_weight, *small)


def solution(mesh):
    placed = (
        P(("rep", "fs"), "tp"),
        P("tp"),
        P("tp", None, "fs"),
        P("tp", None),
        P("tp", "fs"),
        P("tp"),
        P("tp"),
        P("fs", "tp"),
        P("tp"),
        P("fs", "tp"),
        P("tp"),
        P(None, "tp"),
        P("tp", "fs"),
        P("tp"),
    )
    body = functools.partial(per_device, mesh.shape["fs"])
    return jax.shard_map(
        body, mesh=mesh, in_specs=placed, out_specs=P(("rep", "fs"), "tp"), check_vma=False
    )
```
